128 devices in a mesh: sp: 16 (over z, y), dp: 8 (over x, core).
Axes of the slice: x: 4, y: 4, z: 4, core: 2. Of those that a mesh axis runs over, the one named last changes fastest.
Arguments:
- residual: bfloat16 [8, 2048, 2048], P('dp', 'sp'), may hold values from -6 to 6
- query_maps: bfloat16 [8, 2048, 2048], P('dp', 'sp'), may hold values from -200 to 200
- key_maps: bfloat16 [8, 2048, 2048], P('dp', 'sp'), may hold values from -200 to 200
- value_rows: bfloat16 [8, 2048, 2048], P('dp', 'sp'), may hold values from -6 to 6
- lambdas: float32 [16], replicated, may hold values from 0.3 to 0.8
- head_gain: float32 [2048], replicated, may hold values from 0.1 to 1.9
- out_weight: bfloat16 [2048, 2048], replicated, may hold values from -0.125 to 0.125
- ffn_gain: float32 [2048], replicated, may hold values from 0.1 to 1.9
- routes: int32 [8, 2048, 2], P('dp', 'sp'), may hold values from 0 to 127, all different within a row; in each aligned block of 128 rows (0 to 127, 128 to 255, ..., all dimensions but the last counted through in order) at most 4 rows name the same one
- route_weights: float32 [8, 2048, 2], P('dp', 'sp'), may hold values from 0.2 to 1
- expert_gate: bfloat16 [128, 2048, 1024], P(('sp', 'dp')), may hold values from -0.125 to 0.125
- expert_up: bfloat16 [128, 2048, 1024], P(('sp', 'dp')), may hold values from -0.125 to 0.125
- expert_down: bfloat16 [128, 1024, 2048], P(('sp', 'dp')), may hold values from -0.1875 to 0.1875
Outputs:
- layer_out: bfloat16 [8, 2048, 2048], P('dp', 'sp')
The draws below stay inside these ranges and needn't reach their ends.
Inputs may be any that keep to these rules, and one draw needn't show every extreme that they name: `routes`: A token's 2 experts differ; among the 128 rows of one device no expert is named more than 4 times, and in every draw some expert is named exactly 4 times by one device's rows.
All inputs are finite; a program needn't handle non-finite values.
Results may differ from the reference program's by a relative error of at most 0.012.
Values may be sent and summed in bfloat16 or wider, within the bound.
No kernel may reach another device: no remote copies, remote signals or barrier semaphores. Data moves between devices by JAX's collectives and lax.ppermute only.
A program may use at most 128 MiB of HBM per device.

```python
import math
import jax
import jax.numpy as jnp
import numpy as np
from jax import lax

D = 2048
HEADS = 16
HD = 64
VD = 128
FF = 1024
TOPK = 2
TOK_DEV = 128
SEQ = 2048
EXPERTS = 128
CAP = 4
N_DP = 8


def base_keys(key):
    return 1.3 * jax.random.normal(jax.random.fold_in(key, 11), (N_DP, SEQ, HEADS * 2 * HD), jnp.float32)


def draw_key_maps(key, part):
    drawn = base_keys(key)
    return drawn.astype(jnp.bfloat16)


def draw_query_maps(key, part):
    drawn = 1.3 * jax.random.normal(jax.random.fold_in(key, 21), (N_DP, SEQ, HEADS * 2 * HD), jnp.float32)
    return drawn.astype(jnp.bfloat16)


def shard_levels(key, extent, split, least, largest):
    gain = 1.0
    for axis_at, shards_of in split:
        steps = jax.random.uniform(jax.random.fold_in(jax.random.fold_in(key, 6), axis_at), (shards_of,), jnp.float32, least / len(split), largest / len(split))
        gain = gain * jnp.repeat(jnp.exp(steps), extent[axis_at] // shards_of).reshape((-1,) + (1,) * (len(extent) - 1 - axis_at))
    return gain


def shared_out(own_key, own, number, rows, number_of, top, limit, skew):
    sequence = jax.random.permutation(own_key, number_of)
    crowded, usual = load_shares(number_of, rows * top, limit, skew, True), load_shares(number_of, rows * top, limit, skew, False)
    places = jnp.arange(number_of)

    def named(lengths, turn):
        used = int((lengths > 0).sum())
        fixed = max(1, used // 4)
        passed = fixed + (places - fixed + turn * (used - fixed)) % max(1, number_of - fixed)
        return jnp.zeros((number_of,), jnp.int32).at[sequence[jnp.where(places < fixed, places, passed)]].set(jnp.asarray(lengths, jnp.int32))

    lengths = jnp.where(number % 4 == 0, named(crowded, number // 4), named(usual, number - number // 4 - 1))
    mixed = jax.random.permutation(jax.random.fold_in(own, 3), number_of)
    giver, taker = mixed[0:number_of // 2 * 2:2], mixed[1:number_of // 2 * 2:2]
    slack = jnp.minimum(lengths[giver] - 1, limit - lengths[taker]) // 2
    slack = jnp.where((giver == sequence[0]) | (taker == sequence[0]) | (lengths[taker] == 0), 0, jnp.maximum(slack, 0))
    passed = jax.random.randint(jax.random.fold_in(own, 4), (number_of // 2,), 0, 1 << 20) % (slack + 1)
    lengths = lengths.at[giver].add(-passed).at[taker].add(passed)
    members = jnp.searchsorted(jnp.cumsum(lengths), jnp.arange(rows * top), side="right").astype(jnp.int32)
    table = members.reshape(top, rows).T
    table = table[jax.random.permutation(jax.random.fold_in(own, 1), rows)]
    turn = jax.random.randint(jax.random.fold_in(own, 2), (rows, 1), 0, top)
    return jnp.take_along_axis(table, (jnp.arange(top)[None, :] + turn) % top, axis=1)


def load_shares(count, total, bound, slope, full):
    weights = [(1 << 20) // math.isqrt(rank ** slope) + 1 for rank in range(1, count + 1)]
    largest = bound if full else min(bound, max(-(-total // count), total * weights[0] // sum(weights)))
    least = 1 if total - largest >= count - 1 else 0
    holding, spare = [largest] + [least] * (count - 1), total - largest - least * (count - 1)
    while spare > 0:
        candidates = [i for i in range(1, count) if holding[i] < largest] or [i for i in range(1, count) if holding[i] < bound]
        whole, remaining = sum([weights[i] for i in candidates]), spare
        for i in candidates:
            extra = min(bound - holding[i], max(1, remaining * weights[i] // whole), spare)
            holding[i] = holding[i] + extra
            spare = spare - extra
    return np.array(holding)


def scatter_about(rng, extent, scale, bound, shards=(), kind=jnp.bfloat16):
    gain = shard_levels(rng, extent, shards, -0.22, 0.18) if shards else 1.0
    values = jax.random.normal(rng, extent, jnp.float32) * scale * gain
    return jnp.minimum(jnp.maximum(values, -bound), bound).astype(kind)


def setup_inputs(seed: int = 0) -> dict:
    arg_keys = jax.random.split(jax.random.key(seed), 14)
    residual = scatter_about(arg_keys[0], (N_DP, SEQ, D), 1.0, 6.0, ((0, 8), (1, 16)))
    query_maps = draw_query_maps(jax.random.fold_in(arg_keys[13], 71), 0)
    key_maps = draw_key_maps(jax.random.fold_in(arg_keys[13], 71), 0)
    value_rows = scatter_about(arg_keys[3], (N_DP, SEQ, HEADS * VD), 1.0, 6.0, ((0, 8), (1, 16)))
    lambdas = jnp.clip(jax.random.uniform(arg_keys[4], (HEADS,), jnp.float32, 0.3, 0.8), 0.3, 0.8)
    head_gain = jnp.clip(1.0 + 0.18 * jax.random.normal(arg_keys[5], (HEADS * VD,), jnp.float32), 0.1, 1.9)
    out_weight = scatter_about(arg_keys[6], (HEADS * VD, D), (HEADS * VD) ** -0.5, 0.125)
    ffn_gain = jnp.clip(1.0 + 0.18 * jax.random.normal(arg_keys[7], (D,), jnp.float32), 0.1, 1.9)
    routes_keys = jax.random.split(jax.random.fold_in(arg_keys[8], 1), N_DP * SEQ // TOK_DEV)
    routes_turns = jax.random.permutation(jax.random.fold_in(arg_keys[8], 3), N_DP * SEQ // TOK_DEV)
    routes = jax.vmap(lambda own, number: shared_out(jax.random.fold_in(arg_keys[8], 2), own, number, TOK_DEV, EXPERTS, TOPK, CAP, 2))(routes_keys, routes_turns).reshape((N_DP, SEQ, TOPK))
    route_weights = jnp.clip(jnp.exp(math.log(1.0) - 1.609438 * jax.random.uniform(arg_keys[9], (N_DP, SEQ, TOPK), jnp.float32) ** shard_levels(arg_keys[9], (N_DP, SEQ, TOPK), ((0, 8), (1, 16)), -0.2, 0.2)), 0.2, 1.0)
    expert_gate = scatter_about(arg_keys[10], (EXPERTS, D, FF), D ** -0.5, 0.125, ((0, 128),))
    expert_up = scatter_about(arg_keys[11], (EXPERTS, D, FF), D ** -0.5, 0.125, ((0, 128),))
    expert_down = scatter_about(arg_keys[12], (EXPERTS, FF, D), FF ** -0.5, 0.1875, ((0, 128),))
    return {"residual": residual, "query_maps": query_maps, "key_maps": key_maps, "value_rows": value_rows, "lambdas": lambdas, "head_gain": head_gain, "out_weight": out_weight, "ffn_gain": ffn_gain, "routes": routes, "route_weights": route_weights, "expert_gate": expert_gate, "expert_up": expert_up, "expert_down": expert_down}


eps = 1e-06

def attend_head(query_head, key_head, value_head, lam_head, gain_head):
    length = query_head.shape[0]
    block_rows = min(512, length)
    count_blocks = length // block_rows
    scaling = query_head.shape[-1] ** (-0.5)
    query_blocks = query_head.reshape(count_blocks, block_rows, 2, query_head.shape[-1])
    keys_wide = key_head.astype(jnp.float32)

    def one_block(query_block):
        scores = jnp.einsum('qmd,kmd->mqk', query_block.astype(jnp.float32), keys_wide) * scaling
        probabilities = jax.nn.softmax(scores, axis=-1)
        mixed_map = (probabilities[0] - lam_head * probabilities[1]).astype(jnp.bfloat16)
        head_out = jnp.dot(mixed_map, value_head, preferred_element_type=jnp.float32)
        normed = head_out * lax.rsqrt(lax.optimization_barrier(jnp.mean(head_out * head_out, axis=-1, keepdims=True)) + eps)
        return (normed * gain_head * 0.8).astype(jnp.bfloat16)
    return lax.map(one_block, query_blocks).reshape(length, value_head.shape[-1])

def reference(residual, query_maps, key_maps, value_rows, lambdas, head_gain, out_weight, ffn_gain, routes, route_weights, expert_gate, expert_up, expert_down):
    items = N_DP * HEADS
    query_items = query_maps.reshape(N_DP, SEQ, HEADS, 2, HD).transpose(0, 2, 1, 3, 4).reshape(items, SEQ, 2, HD)
    key_items = key_maps.reshape(N_DP, SEQ, HEADS, 2, HD).transpose(0, 2, 1, 3, 4).reshape(items, SEQ, 2, HD)
    value_items = value_rows.reshape(N_DP, SEQ, HEADS, VD).transpose(0, 2, 1, 3).reshape(items, SEQ, VD)
    lam_items = jnp.tile(lambdas, N_DP)
    gain_items = jnp.tile(head_gain.reshape(HEADS, VD), (N_DP, 1))

    def per_item(packed):
        return attend_head(packed[0], packed[1], packed[2], packed[3], packed[4])
    attended = lax.map(per_item, (query_items, key_items, value_items, lam_items, gain_items))
    attended = attended.reshape(N_DP, HEADS, SEQ, VD).transpose(0, 2, 1, 3).reshape(N_DP * SEQ, HEADS * VD)
    total_rows = N_DP * SEQ
    projected = jnp.dot(attended, out_weight, preferred_element_type=jnp.float32)
    residual_mid = (residual.reshape(total_rows, D).astype(jnp.float32) + projected).astype(jnp.bfloat16)
    middle = residual_mid.astype(jnp.float32)
    expert_input = (middle * lax.rsqrt(lax.optimization_barrier(jnp.mean(middle * middle, axis=-1, keepdims=True)) + eps) * ffn_gain).astype(jnp.bfloat16)
    count_blocks = total_rows // TOK_DEV
    block_routes = routes.reshape(count_blocks, TOK_DEV * TOPK)

    def rank_block(route_block):
        onehot = (route_block[:, None] == jnp.arange(EXPERTS, dtype=jnp.int32)[None, :]).astype(jnp.int32)
        before = jnp.cumsum(onehot, axis=0) - onehot
        return lax.optimization_barrier(jnp.sum(before * onehot, axis=1))
    rank_of = lax.map(rank_block, block_routes).reshape(-1)
    flat_routes = routes.reshape(-1).astype(jnp.int32)
    token_of = (jnp.arange(total_rows * TOPK, dtype=jnp.int32) // TOPK).astype(jnp.int32)
    column = token_of // TOK_DEV * CAP + rank_of
    slot_table = jnp.full((EXPERTS, count_blocks * CAP), total_rows, jnp.int32).at[flat_routes, column].set(token_of)
    weight_table = jnp.zeros((EXPERTS, count_blocks * CAP), jnp.float32).at[flat_routes, column].set(route_weights.reshape(-1))
    padded_input = jnp.concatenate([expert_input, jnp.zeros((1, D), jnp.bfloat16)], axis=0)

    def per_expert(accumulated, packed):
        table_row, weight_row, gate_weight, up_weight, down_weight = packed
        row_block = padded_input[table_row]
        gate_part = jnp.dot(row_block, gate_weight, preferred_element_type=jnp.float32)
        up_part = jnp.dot(row_block, up_weight, preferred_element_type=jnp.float32)
        hidden = (jax.nn.silu(gate_part) * up_part).astype(jnp.bfloat16)
        expert_out = jnp.dot(hidden, down_weight, preferred_element_type=jnp.float32).astype(jnp.bfloat16)
        accumulated = accumulated.at[table_row].add(weight_row[:, None] * expert_out.astype(jnp.float32))
        return (accumulated, None)
    start_sum = jnp.zeros((total_rows + 1, D), jnp.float32)
    accumulated, _ = lax.scan(per_expert, start_sum, (slot_table, weight_table, expert_gate, expert_up, expert_down))
    layer_out = (middle + accumulated[:total_rows]).astype(jnp.bfloat16)
    return layer_out.reshape(N_DP, SEQ, D)
```

```python
import math

import jax
import jax.numpy as jnp
from jax import lax
from jax.experimental import pallas as pl
from jax.experimental.pallas import tpu as pltpu
from jax.sharding import Mesh
from jax.sharding import PartitionSpec as P

D = 2048
HEADS = 16
HD = 64
VD = 128
SP = ("sp_0", "sp_1")
SP_DP = ("sp_0", "sp_1", "dp")


eps = 1e-06


def in_blocks(value, dim, size):
    lengths = value.shape
    blocks = value.reshape(*lengths[:dim], size, lengths[dim] // size, *lengths[dim + 1 :])
    return jnp.moveaxis(blocks, dim, 0)


def laid_out(blocks, dim):
    blocks = jnp.moveaxis(blocks, 0, dim)
    lengths = blocks.shape
    return blocks.reshape(*lengths[:dim], lengths[dim] * lengths[dim + 1], *lengths[dim + 2 :])


def exchange_both(value, axis, axes, splits, concats):
    sizes = [lax.axis_size(a) for a in axes]
    blocks = in_blocks(value, splits[0], sizes[0])
    blocks = jnp.moveaxis(in_blocks(blocks, splits[1] + 1, sizes[1]), 0, 1)
    inside = blocks.shape[2:]
    blocks = blocks.reshape(-1, *inside)
    blocks = lax.all_to_all(blocks, axis, split_axis=0, concat_axis=0, tiled=True)
    blocks = laid_out(blocks.reshape(*sizes, *inside), concats[0] + 1)
    return laid_out(blocks, concats[1])


EXP_SCALE = HD ** (-0.5) * math.log2(math.e)
LAST_DIMS = (((1,), (1,)), ((), ()))
ATT_BLOCKS = 2


def attention_kernel(lam_ref, qkv_ref, gain_ref, out_ref, values_ref, scores_ref):
    sources, _, tokens, width = qkv_ref.shape
    length = sources * tokens
    rows = ATT_BLOCKS * tokens
    steps = sources // ATT_BLOCKS
    values_ref[:, :VD] = qkv_ref[:, 2].reshape(length, width)
    values_ref[:, VD:] = jnp.ones((length, VD), jnp.bfloat16)

    def scores(step, slot):
        keys = qkv_ref[:, 1].reshape(length, width)
        query = qkv_ref[pl.ds(step * ATT_BLOCKS, ATT_BLOCKS), 0].reshape(rows, width)
        lane = lax.broadcasted_iota(jnp.int32, query.shape, 1)
        zero = jnp.zeros_like(query)
        both = jnp.concatenate(
            [jnp.where(lane < HD, query, zero), jnp.where(lane < HD, zero, query)], axis=0
        )
        scores_ref[slot] = lax.dot_general(
            both, keys, LAST_DIMS, preferred_element_type=jnp.float32
        )

    def attend(step, slot):
        score = scores_ref[slot]
        top = jnp.max(score, axis=-1, keepdims=True)
        weight = jnp.exp2((score - top) * EXP_SCALE).astype(jnp.bfloat16)
        summed = jnp.dot(weight, values_ref[...], preferred_element_type=jnp.float32)
        first, second = summed[:rows], summed[rows:]
        head_out = first[:, :VD] / first[:, VD:] - lam_ref[0] * (second[:, :VD] / second[:, VD:])
        normed = head_out * lax.rsqrt(jnp.mean(head_out * head_out, axis=-1, keepdims=True) + eps)
        out_ref[pl.ds(step * ATT_BLOCKS, ATT_BLOCKS)] = (
            (normed * gain_ref[...] * 0.8).astype(jnp.bfloat16).reshape(ATT_BLOCKS, tokens, VD)
        )

    scores(0, 0)

    def pair(index, carry):
        scores(2 * index + 1, 1)
        attend(2 * index, 0)
        scores(2 * index + 2, 0)
        attend(2 * index + 1, 1)
        return carry

    lax.fori_loop(0, steps // 2 - 1, pair, 0)
    scores(steps - 1, 1)
    attend(steps - 2, 0)
    attend(steps - 1, 1)


def attention(lam, qkv, gain):
    sources, _, tokens, width = qkv.shape
    length = sources * tokens
    in_vmem = pl.BlockSpec(memory_space=pltpu.VMEM)
    return pl.pallas_call(
        attention_kernel,
        in_specs=[pl.BlockSpec(memory_space=pltpu.SMEM), in_vmem, in_vmem],
        out_specs=in_vmem,
        out_shape=jax.ShapeDtypeStruct((sources, tokens, VD), jnp.bfloat16),
        scratch_shapes=[
            pltpu.VMEM((length, 2 * VD), jnp.bfloat16),
            pltpu.VMEM((2, 2 * ATT_BLOCKS * tokens, length), jnp.float32),
        ],
        name="attention",
    )(lam, qkv, gain)


def on_device(
    residual,
    query_maps,
    key_maps,
    value_rows,
    lambdas,
    head_gain,
    out_weight,
    ffn_gain,
    routes,
    route_weights,
    expert_gate,
    expert_up,
    expert_down,
):
    count_sp = lax.axis_size(SP)
    count_dp = lax.axis_size("dp")
    tokens = residual.shape[1]
    packed = jnp.stack([query_maps[0], key_maps[0], value_rows[0]])
    packed = packed.reshape(3, tokens, count_sp, VD).transpose(2, 0, 1, 3)
    qkv = lax.all_to_all(packed, SP, split_axis=0, concat_axis=0, tiled=True)
    head = lax.axis_index(SP)
    lam_here = lax.dynamic_slice_in_dim(lambdas, head, 1)
    gain_here = lax.dynamic_slice_in_dim(head_gain, head * VD, VD)[None]
    attended = attention(lam_here, qkv, gain_here)
    returned = lax.all_to_all(attended, SP, split_axis=0, concat_axis=0, tiled=True)
    returned_heads = returned.transpose(1, 0, 2).reshape(tokens, HEADS * VD)
    projected = jnp.dot(returned_heads, out_weight, preferred_element_type=jnp.float32)
    residual_mid = (residual[0].astype(jnp.float32) + projected).astype(jnp.bfloat16)
    middle = residual_mid.astype(jnp.float32)
    expert_input = (
        middle * lax.rsqrt(jnp.mean(middle * middle, axis=-1, keepdims=True) + eps) * ffn_gain
    ).astype(jnp.bfloat16)
    tok_rows = residual.shape[1]
    experts_all = count_sp * count_dp
    capacity = max(2, 4 * tok_rows // experts_all)
    flat_routes = routes[0].reshape(-1)
    flat_weights = route_weights[0].reshape(-1)
    onehot = (flat_routes[:, None] == jnp.arange(experts_all, dtype=jnp.int32)[None, :]).astype(
        jnp.int32
    )
    before = jnp.cumsum(onehot, axis=0) - onehot
    rank_of = jnp.sum(before * onehot, axis=1)
    slot = flat_routes * capacity + rank_of
    token_of = jnp.arange(flat_routes.shape[0], dtype=jnp.int32) // routes.shape[2]
    slot_token = jnp.full((experts_all * capacity,), tok_rows, jnp.int32).at[slot].set(token_of)
    padded_input = jnp.concatenate([expert_input, jnp.zeros((1, D), jnp.bfloat16)], axis=0)
    buffer = padded_input[slot_token].reshape(experts_all, capacity, D)
    shaped = buffer.reshape(count_sp, count_dp, capacity, D)
    received = exchange_both(shaped, SP_DP, (SP, "dp"), (0, 1), (0, 1))
    row_block = received.reshape(-1, D)
    gate_part = jnp.dot(row_block, expert_gate[0], preferred_element_type=jnp.float32)
    up_part = jnp.dot(row_block, expert_up[0], preferred_element_type=jnp.float32)
    hidden = (jax.nn.silu(gate_part) * up_part).astype(jnp.bfloat16)
    expert_out = jnp.dot(hidden, expert_down[0], preferred_element_type=jnp.float32).astype(
        jnp.bfloat16
    )
    returned = exchange_both(expert_out.reshape(received.shape), SP_DP, (SP, "dp"), (0, 1), (0, 1))
    picked = returned.reshape(experts_all * capacity, D)[slot]
    weighted = (picked.astype(jnp.float32) * flat_weights[:, None]).reshape(
        tok_rows, routes.shape[2], D
    )
    layer_out = (middle + jnp.sum(weighted, axis=1)).astype(jnp.bfloat16)
    return layer_out[None]


def solution(mesh):
    finer = Mesh(mesh.devices.reshape(4, 4, mesh.shape["dp"]), ("sp_0", "sp_1", "dp"))
    placed = (
        P("dp", SP, None),
        P("dp", SP, None),
        P("dp", SP, None),
        P("dp", SP, None),
        P(),
        P(),
        P(),
        P(),
        P("dp", SP, None),
        P("dp", SP, None),
        P(SP_DP, None, None),
        P(SP_DP, None, None),
        P(SP_DP, None, None),
    )
    return jax.shard_map(
        on_device, mesh=finer, in_specs=placed, out_specs=P("dp", SP, None), check_vma=False
    )
```

```python
import math

import jax
import jax.numpy as jnp
from jax import lax
from jax.experimental import pallas as pl
from jax.experimental.pallas import tpu as pltpu
from jax.sharding import Mesh
from jax.sharding import PartitionSpec as P

D = 2048
HEADS = 16
HD = 64
VD = 128
SP = ("sp_0", "sp_1")
SP_DP = ("sp_0", "sp_1", "dp")


eps = 1e-06


EXP_SCALE = HD ** (-0.5) * math.log2(math.e)
LAST_DIMS = (((1,), (1,)), ((), ()))
ATT_BLOCKS = 2


def attention_kernel(lam_ref, qkv_ref, gain_ref, out_ref, values_ref, scores_ref):
    sources, _, tokens, width = qkv_ref.shape
    length = sources * tokens
    rows = ATT_BLOCKS * tokens
    steps = sources // ATT_BLOCKS
    values_ref[:, :VD] = qkv_ref[:, 2].reshape(length, width)
    values_ref[:, VD:] = jnp.ones((length, VD), jnp.bfloat16)

    def scores(step, slot):
        keys = qkv_ref[:, 1].reshape(length, width)
        query = qkv_ref[pl.ds(step * ATT_BLOCKS, ATT_BLOCKS), 0].reshape(rows, width)
        lane = lax.broadcasted_iota(jnp.int32, query.shape, 1)
        zero = jnp.zeros_like(query)
        both = jnp.concatenate(
            [jnp.where(lane < HD, query, zero), jnp.where(lane < HD, zero, query)], axis=0
        )
        scores_ref[slot] = lax.dot_general(
            both, keys, LAST_DIMS, preferred_element_type=jnp.float32
        )

    def attend(step, slot):
        score = scores_ref[slot]
        top = jnp.max(score, axis=-1, keepdims=True)
        weight = jnp.exp2((score - top) * EXP_SCALE).astype(jnp.bfloat16)
        summed = jnp.dot(weight, values_ref[...], preferred_element_type=jnp.float32)
        first, second = summed[:rows], summed[rows:]
        head_out = first[:, :VD] / first[:, VD:] - lam_ref[0] * (second[:, :VD] / second[:, VD:])
        normed = head_out * lax.rsqrt(jnp.mean(head_out * head_out, axis=-1, keepdims=True) + eps)
        out_ref[pl.ds(step * ATT_BLOCKS, ATT_BLOCKS)] = (
            (normed * gain_ref[...] * 0.8).astype(jnp.bfloat16).reshape(ATT_BLOCKS, tokens, VD)
        )

    scores(0, 0)

    def pair(index, carry):
        scores(2 * index + 1, 1)
        attend(2 * index, 0)
        scores(2 * index + 2, 0)
        attend(2 * index + 1, 1)
        return carry

    lax.fori_loop(0, steps // 2 - 1, pair, 0)
    scores(steps - 1, 1)
    attend(steps - 2, 0)
    attend(steps - 1, 1)


def attention(lam, qkv, gain):
    sources, _, tokens, width = qkv.shape
    length = sources * tokens
    in_vmem = pl.BlockSpec(memory_space=pltpu.VMEM)
    return pl.pallas_call(
        attention_kernel,
        in_specs=[pl.BlockSpec(memory_space=pltpu.SMEM), in_vmem, in_vmem],
        out_specs=in_vmem,
        out_shape=jax.ShapeDtypeStruct((sources, tokens, VD), jnp.bfloat16),
        scratch_shapes=[
            pltpu.VMEM((length, 2 * VD), jnp.bfloat16),
            pltpu.VMEM((2, 2 * ATT_BLOCKS * tokens, length), jnp.float32),
        ],
        name="attention",
    )(lam, qkv, gain)


ROW = (16, 128)
GROUP = 16
CAP = 4
HALVES = 2
CAP_HALF = CAP // HALVES


def route_kernel(routes_ref, slot_ref, token_ref, count_ref):
    experts = count_ref.shape[0]
    slots = token_ref.shape[0]

    def clear_count(index, carry):
        count_ref[index] = 0
        return carry

    def clear_token(index, carry):
        token_ref[index] = 0
        return carry

    def place(index, carry):
        expert = routes_ref[index]
        rank = count_ref[expert]
        count_ref[expert] = rank + 1
        slot = (rank // CAP_HALF) * (experts * CAP_HALF) + expert * CAP_HALF + rank % CAP_HALF
        slot_ref[index] = slot
        token_ref[slot] = index // 2
        return carry

    lax.fori_loop(0, experts, clear_count, 0, unroll=8)
    lax.fori_loop(0, slots, clear_token, 0, unroll=8)
    lax.fori_loop(0, slot_ref.shape[0], place, 0)


def route_slots(flat_routes, experts):
    in_smem = pl.BlockSpec(memory_space=pltpu.SMEM)
    return pl.pallas_call(
        route_kernel,
        in_specs=[in_smem],
        out_specs=[in_smem, in_smem],
        out_shape=[
            jax.ShapeDtypeStruct(flat_routes.shape, jnp.int32),
            jax.ShapeDtypeStruct((experts * CAP,), jnp.int32),
        ],
        scratch_shapes=[pltpu.SMEM((experts,), jnp.int32)],
        name="route_slots",
    )(flat_routes)


def swap_matrix():
    size = GROUP * GROUP
    to = lax.broadcasted_iota(jnp.int32, (size, size), 0)
    at = lax.broadcasted_iota(jnp.int32, (size, size), 1)
    same = (to % GROUP) * GROUP + to // GROUP == at
    return jnp.where(same, 1.0, 0.0).astype(jnp.bfloat16)


def rows_to_tiles(rows, swap):
    blocks = [rows[:, 128 * j : 128 * (j + 1)] for j in range(16)]
    stacked = jnp.concatenate(blocks, axis=0)
    swapped = jnp.dot(swap, stacked, preferred_element_type=jnp.float32)
    return swapped.astype(jnp.bfloat16).reshape(GROUP, *ROW)


def tiles_to_rows(tiles, swap):
    stacked = tiles.reshape(GROUP * GROUP, 128)
    swapped = jnp.dot(swap, stacked, preferred_element_type=jnp.float32).astype(jnp.bfloat16)
    return jnp.concatenate([swapped[GROUP * j : GROUP * (j + 1)] for j in range(16)], axis=1)


def middle_kernel(
    token_ref, heads_ref, weight_ref, residual_ref, gain_ref,
    mid_ref, first_ref, second_ref, heads_rows, middle, tiles,
):
    step = pl.program_id(0)
    width = weight_ref.shape[1]
    tokens = middle.shape[0]

    @pl.when(step == 0)
    def _():
        for head in range(HEADS):
            heads_rows[:, head * VD : (head + 1) * VD] = heads_ref[head]

    projected = jnp.dot(heads_rows[...], weight_ref[...], preferred_element_type=jnp.float32)
    at = pl.multiple_of(step * width, width)
    middle[:, pl.ds(at, width)] = (residual_ref[...].astype(jnp.float32) + projected).astype(
        jnp.bfloat16
    )

    @pl.when(step == pl.num_programs(0) - 1)
    def _():
        swap = swap_matrix()
        for group in range(tokens // GROUP):
            rows = slice(group * GROUP, (group + 1) * GROUP)
            mid = middle[rows, :]
            mid_ref[rows] = rows_to_tiles(mid, swap)
            wide = mid.astype(jnp.float32)
            scale = lax.rsqrt(jnp.mean(wide * wide, axis=-1, keepdims=True) + eps)
            expert_input = (wide * scale * gain_ref[...]).astype(jnp.bfloat16)
            tiles[rows] = rows_to_tiles(expert_input, swap)

        half = first_ref.shape[0]

        def gather(index, carry):
            first_ref[index] = tiles[token_ref[index]]
            second_ref[index] = tiles[token_ref[half + index]]
            return carry

        lax.fori_loop(0, half, gather, 0, unroll=8)


def middle_stage(slot_token, heads, out_weight, residual, gain):
    tokens = residual.shape[0]
    half = slot_token.shape[0] // HALVES
    block = 512
    whole = lambda *lengths: pl.BlockSpec(lengths, lambda i: (0,) * len(lengths))
    return pl.pallas_call(
        middle_kernel,
        grid=(D // block,),
        in_specs=[
            pl.BlockSpec(memory_space=pltpu.SMEM),
            whole(HEADS, tokens, VD),
            pl.BlockSpec((HEADS * VD, block), lambda i: (0, i)),
            pl.BlockSpec((tokens, block), lambda i: (0, i)),
            whole(1, D),
        ],
        out_specs=[whole(tokens, *ROW), whole(half, *ROW), whole(half, *ROW)],
        out_shape=[
            jax.ShapeDtypeStruct((tokens, *ROW), jnp.bfloat16),
            jax.ShapeDtypeStruct((half, *ROW), jnp.bfloat16),
            jax.ShapeDtypeStruct((half, *ROW), jnp.bfloat16),
        ],
        scratch_shapes=[
            pltpu.VMEM((tokens, D), jnp.bfloat16),
            pltpu.VMEM((tokens, D), jnp.bfloat16),
            pltpu.VMEM((tokens, *ROW), jnp.bfloat16),
        ],
        cost_estimate=pl.CostEstimate(
            flops=2 * tokens * D * D, bytes_accessed=2 * D * D, transcendentals=0
        ),
        name="middle",
    )(slot_token, heads, out_weight, residual, gain)


def expert_kernel(tile_ref, gate_ref, up_ref, down_ref, out_ref, rows, total):
    step = pl.program_id(0)
    groups = tile_ref.shape[0] // GROUP

    @pl.when(step == 0)
    def _():
        swap = swap_matrix()
        for group in range(groups):
            at = slice(group * GROUP, (group + 1) * GROUP)
            rows[at, :] = tiles_to_rows(tile_ref[at], swap)

    inputs = rows[...]
    gate = jnp.dot(inputs, gate_ref[0], preferred_element_type=jnp.float32)
    up = jnp.dot(inputs, up_ref[0], preferred_element_type=jnp.float32)
    hidden = (gate / (1.0 + jnp.exp(-gate)) * up).astype(jnp.bfloat16)
    part = jnp.dot(hidden, down_ref[0], preferred_element_type=jnp.float32)

    @pl.when(step == 0)
    def _():
        total[...] = part

    @pl.when(step > 0)
    def _():
        total[...] += part

    @pl.when(step == pl.num_programs(0) - 1)
    def _():
        swap = swap_matrix()
        for group in range(groups):
            at = slice(group * GROUP, (group + 1) * GROUP)
            out_ref[at] = rows_to_tiles(total[at, :].astype(jnp.bfloat16), swap)


def expert_stage(tiles, gate, up, down):
    count = tiles.shape[0]
    hidden = gate.shape[2]
    block = 256
    whole = pl.BlockSpec((count, *ROW), lambda i: (0, 0, 0))
    columns = pl.BlockSpec((1, D, block), lambda i: (0, 0, i))
    return pl.pallas_call(
        expert_kernel,
        grid=(hidden // block,),
        in_specs=[whole, columns, columns, pl.BlockSpec((1, block, D), lambda i: (0, i, 0))],
        out_specs=whole,
        out_shape=jax.ShapeDtypeStruct((count, *ROW), jnp.bfloat16),
        scratch_shapes=[pltpu.VMEM((count, D), jnp.bfloat16), pltpu.VMEM((count, D), jnp.float32)],
        cost_estimate=pl.CostEstimate(
            flops=6 * count * D * hidden, bytes_accessed=6 * D * hidden, transcendentals=0
        ),
        name="experts",
    )(tiles, gate, up, down)


def combine_kernel(slot_ref, share_ref, mid_ref, first_hbm, second_hbm, out_ref, back, tiles, sems):
    half = first_hbm.shape[0]
    tokens = mid_ref.shape[0]
    copies = [
        pltpu.make_async_copy(source, back.at[pl.ds(n * half, half)], sems.at[n])
        for n, source in enumerate((first_hbm, second_hbm))
    ]
    for copy in copies:
        copy.start()
    for copy in copies:
        copy.wait()

    def token(index, carry):
        one = back[slot_ref[2 * index]].astype(jnp.float32) * share_ref[2 * index]
        two = back[slot_ref[2 * index + 1]].astype(jnp.float32) * share_ref[2 * index + 1]
        tiles[index] = (mid_ref[index].astype(jnp.float32) + (one + two)).astype(jnp.bfloat16)
        return carry

    lax.fori_loop(0, tokens, token, 0, unroll=8)
    swap = swap_matrix()
    for group in range(tokens // GROUP):
        at = slice(group * GROUP, (group + 1) * GROUP)
        out_ref[at, :] = tiles_to_rows(tiles[at], swap)


def combine_stage(slot, shares, mid, first, second):
    tokens = mid.shape[0]
    half = first.shape[0]
    in_smem = pl.BlockSpec(memory_space=pltpu.SMEM)
    in_vmem = pl.BlockSpec(memory_space=pltpu.VMEM)
    in_place = pl.BlockSpec(memory_space=pl.ANY)
    return pl.pallas_call(
        combine_kernel,
        in_specs=[in_smem, in_smem, in_vmem, in_place, in_place],
        out_specs=in_vmem,
        out_shape=jax.ShapeDtypeStruct((tokens, D), jnp.bfloat16),
        scratch_shapes=[
            pltpu.VMEM((HALVES * half, *ROW), jnp.bfloat16),
            pltpu.VMEM((tokens, *ROW), jnp.bfloat16),
            pltpu.SemaphoreType.DMA((HALVES,)),
        ],
        name="combine",
    )(slot, shares, mid, first, second)


def on_device(
    residual,
    query_maps,
    key_maps,
    value_rows,
    lambdas,
    head_gain,
    out_weight,
    ffn_gain,
    routes,
    route_weights,
    expert_gate,
    expert_up,
    expert_down,
):
    count_sp = lax.axis_size(SP)
    count_dp = lax.axis_size("dp")
    tokens = residual.shape[1]
    packed = jnp.stack([query_maps[0], key_maps[0], value_rows[0]])
    packed = packed.reshape(3, tokens, count_sp, VD).transpose(2, 0, 1, 3)
    qkv = lax.all_to_all(packed, SP, split_axis=0, concat_axis=0, tiled=True)
    head = lax.axis_index(SP)
    lam_here = lax.dynamic_slice_in_dim(lambdas, head, 1)
    gain_here = lax.dynamic_slice_in_dim(head_gain, head * VD, VD)[None]
    attended = attention(lam_here, qkv, gain_here)
    returned = lax.all_to_all(attended, SP, split_axis=0, concat_axis=0, tiled=True)
    experts_all = count_sp * count_dp
    slot, slot_token = route_slots(routes[0].reshape(-1), experts_all)
    mid, *sent = middle_stage(slot_token, returned, out_weight, residual[0], ffn_gain[None])
    back = []
    for part in sent:
        arrived = lax.all_to_all(part, SP_DP, split_axis=0, concat_axis=0, tiled=True)
        done = expert_stage(arrived, expert_gate, expert_up, expert_down)
        back.append(lax.all_to_all(done, SP_DP, split_axis=0, concat_axis=0, tiled=True))
    return combine_stage(slot, route_weights[0].reshape(-1), mid, *back)[None]


def solution(mesh):
    finer = Mesh(mesh.devices.reshape(4, 4, mesh.shape["dp"]), ("sp_0", "sp_1", "dp"))
    placed = (
        P("dp", SP, None),
        P("dp", SP, None),
        P("dp", SP, None),
        P("dp", SP, None),
        P(),
        P(),
        P(),
        P(),
        P("dp", SP, None),
        P("dp", SP, None),
        P(SP_DP, None, None),
        P(SP_DP, None, None),
        P(SP_DP, None, None),
    )
    return jax.shard_map(
        on_device, mesh=finer, in_specs=placed, out_specs=P("dp", SP, None), check_vma=False
    )
```

```python
import math

import jax
import jax.numpy as jnp
from jax import lax
from jax.experimental import pallas as pl
from jax.experimental.pallas import tpu as pltpu
from jax.sharding import Mesh
from jax.sharding import PartitionSpec as P

D = 2048
HEADS = 16
HD = 64
VD = 128
SP = ("sp_0", "sp_1")
SP_DP = ("sp_0", "sp_1", "dp")


eps = 1e-06


def on_chip(value):
    return pltpu.with_memory_space_constraint(value, pltpu.VMEM)


def within(mebibytes):
    return pltpu.CompilerParams(vmem_limit_bytes=mebibytes * 2**20)


EXP_SCALE = HD ** (-0.5) * math.log2(math.e)
LAST_DIMS = (((1,), (1,)), ((), ()))
ATT_BLOCKS = 2


def attention_kernel(lam_ref, qkv_ref, gain_ref, out_ref, values_ref, scores_ref):
    sources, _, tokens, width = qkv_ref.shape
    length = sources * tokens
    rows = ATT_BLOCKS * tokens
    steps = sources // ATT_BLOCKS
    values_ref[:, :VD] = qkv_ref[:, 2].reshape(length, width)
    values_ref[:, VD:] = jnp.ones((length, VD), jnp.bfloat16)

    def scores(step, slot):
        keys = qkv_ref[:, 1].reshape(length, width)
        query = qkv_ref[pl.ds(step * ATT_BLOCKS, ATT_BLOCKS), 0].reshape(rows, width)
        lane = lax.broadcasted_iota(jnp.int32, query.shape, 1)
        zero = jnp.zeros_like(query)
        both = jnp.concatenate(
            [jnp.where(lane < HD, query, zero), jnp.where(lane < HD, zero, query)], axis=0
        )
        scores_ref[slot] = lax.dot_general(
            both, keys, LAST_DIMS, preferred_element_type=jnp.float32
        )

    def attend(step, slot):
        score = scores_ref[slot]
        top = jnp.max(score, axis=-1, keepdims=True)
        weight = jnp.exp2((score - top) * EXP_SCALE).astype(jnp.bfloat16)
        summed = jnp.dot(weight, values_ref[...], preferred_element_type=jnp.float32)
        first, second = summed[:rows], summed[rows:]
        head_out = first[:, :VD] / first[:, VD:] - lam_ref[0] * (second[:, :VD] / second[:, VD:])
        normed = head_out * lax.rsqrt(jnp.mean(head_out * head_out, axis=-1, keepdims=True) + eps)
        out_ref[pl.ds(step * ATT_BLOCKS, ATT_BLOCKS)] = (
            (normed * gain_ref[...] * 0.8).astype(jnp.bfloat16).reshape(ATT_BLOCKS, tokens, VD)
        )

    scores(0, 0)

    def pair(index, carry):
        scores(2 * index + 1, 1)
        attend(2 * index, 0)
        scores(2 * index + 2, 0)
        attend(2 * index + 1, 1)
        return carry

    lax.fori_loop(0, steps // 2 - 1, pair, 0)
    scores(steps - 1, 1)
    attend(steps - 2, 0)
    attend(steps - 1, 1)


def attention(lam, qkv, gain):
    sources, _, tokens, width = qkv.shape
    length = sources * tokens
    in_vmem = pl.BlockSpec(memory_space=pltpu.VMEM)
    return pl.pallas_call(
        attention_kernel,
        in_specs=[pl.BlockSpec(memory_space=pltpu.SMEM), in_vmem, in_vmem],
        out_specs=in_vmem,
        out_shape=jax.ShapeDtypeStruct((sources, tokens, VD), jnp.bfloat16),
        scratch_shapes=[
            pltpu.VMEM((length, 2 * VD), jnp.bfloat16),
            pltpu.VMEM((2, 2 * ATT_BLOCKS * tokens, length), jnp.float32),
        ],
        compiler_params=within(24),
        cost_estimate=pl.CostEstimate(
            flops=8 * length * length * VD,
            bytes_accessed=8 * length * VD,
            transcendentals=2 * length * length,
        ),
        name="attention",
    )(lam, on_chip(qkv), gain)


ROW = (16, 128)
GROUP = 16
PAIR = 2 * GROUP
CAP = 4


def pack_kernel(query_ref, key_ref, value_ref, out_ref):
    for at, ref in enumerate((query_ref, key_ref, value_ref)):
        for head in range(HEADS):
            out_ref[head, at] = ref[:, head * VD : (head + 1) * VD]


def pack_heads(query, key, value):
    in_vmem = pl.BlockSpec(memory_space=pltpu.VMEM)
    return pl.pallas_call(
        pack_kernel,
        in_specs=[in_vmem] * 3,
        out_specs=in_vmem,
        out_shape=jax.ShapeDtypeStruct((HEADS, 3, query.shape[0], VD), jnp.bfloat16),
        compiler_params=within(8),
        name="pack_heads",
    )(*(pltpu.with_memory_space_constraint(a, pltpu.HBM) for a in (query, key, value)))


def route_kernel(routes_ref, slot_ref, token_ref, count_ref):
    experts = count_ref.shape[0]
    slots = token_ref.shape[0]

    def clear_count(index, carry):
        count_ref[index] = 0
        return carry

    def clear_token(index, carry):
        token_ref[index] = 0
        return carry

    def place(index, carry):
        expert = routes_ref[index]
        rank = count_ref[expert]
        count_ref[expert] = rank + 1
        slot = expert * CAP + rank
        slot_ref[index] = slot
        token_ref[slot] = index // 2
        return carry

    lax.fori_loop(0, experts, clear_count, 0, unroll=8)
    lax.fori_loop(0, slots, clear_token, 0, unroll=8)
    lax.fori_loop(0, slot_ref.shape[0], place, 0)


def route_slots(flat_routes, experts):
    in_smem = pl.BlockSpec(memory_space=pltpu.SMEM)
    return pl.pallas_call(
        route_kernel,
        in_specs=[in_smem],
        out_specs=[in_smem, in_smem],
        out_shape=[
            jax.ShapeDtypeStruct(flat_routes.shape, jnp.int32),
            jax.ShapeDtypeStruct((experts * CAP,), jnp.int32),
        ],
        scratch_shapes=[pltpu.SMEM((experts,), jnp.int32)],
        compiler_params=within(1),
        name="route_slots",
    )(flat_routes)


def swap_matrix():
    size = GROUP * GROUP
    to = lax.broadcasted_iota(jnp.int32, (size, size), 0)
    at = lax.broadcasted_iota(jnp.int32, (size, size), 1)
    same = (to % GROUP) * GROUP + to // GROUP == at
    return jnp.where(same, 1.0, 0.0).astype(jnp.bfloat16)


def rows_to_tiles(rows, swap):
    halves = [
        jnp.concatenate(
            [rows[at : at + GROUP, 128 * j : 128 * (j + 1)] for j in range(16)], axis=0
        )
        for at in (0, GROUP)
    ]
    both = jnp.concatenate(halves, axis=1)
    swapped = jnp.dot(swap, both, preferred_element_type=jnp.float32).astype(jnp.bfloat16)
    return swapped[:, :128].reshape(GROUP, *ROW), swapped[:, 128:].reshape(GROUP, *ROW)


def tiles_to_rows(first, second, swap):
    size = GROUP * GROUP
    both = jnp.concatenate([first.reshape(size, 128), second.reshape(size, 128)], axis=1)
    swapped = jnp.dot(swap, both, preferred_element_type=jnp.float32).astype(jnp.bfloat16)
    return [
        jnp.concatenate(
            [swapped[GROUP * j : GROUP * (j + 1), at : at + 128] for j in range(16)], axis=1
        )
        for at in (0, 128)
    ]


def pair_slices(count):
    for at in range(0, count, PAIR):
        yield slice(at, at + GROUP), slice(at + GROUP, at + PAIR)


def middle_kernel(
    token_ref, heads_ref, weight_ref, residual_ref, gain_ref,
    mid_ref, sent_ref, heads_rows, middle, tiles,
):
    tokens = middle.shape[0]
    block = 512
    for head in range(HEADS):
        heads_rows[:, head * VD : (head + 1) * VD] = heads_ref[head]
    rows = heads_rows[...]
    squares = jnp.zeros((tokens, 128), jnp.float32)
    for at in range(0, D, block):
        columns = slice(at, at + block)
        projected = jnp.dot(rows, weight_ref[:, columns], preferred_element_type=jnp.float32)
        mid = (residual_ref[:, columns].astype(jnp.float32) + projected).astype(jnp.bfloat16)
        middle[:, columns] = mid
        wide = mid.astype(jnp.float32)
        wide = wide * wide
        for lane in range(0, block, 128):
            squares = squares + wide[:, lane : lane + 128]
    scale = lax.rsqrt(jnp.sum(squares, axis=-1, keepdims=True) / D + eps)
    swap = swap_matrix()
    for one, two in pair_slices(tokens):
        both = slice(one.start, two.stop)
        mid = middle[both, :]
        mid_ref[one], mid_ref[two] = rows_to_tiles(mid, swap)
        normed = mid.astype(jnp.float32) * scale[both] * gain_ref[...]
        tiles[one], tiles[two] = rows_to_tiles(normed.astype(jnp.bfloat16), swap)

    def gather(index, carry):
        sent_ref[index] = tiles[token_ref[index]]
        return carry

    lax.fori_loop(0, sent_ref.shape[0], gather, 0, unroll=16)


def middle_stage(slot_token, heads, out_weight, residual, gain):
    tokens = residual.shape[0]
    slots = slot_token.shape[0]
    in_vmem = pl.BlockSpec(memory_space=pltpu.VMEM)
    return pl.pallas_call(
        middle_kernel,
        in_specs=[pl.BlockSpec(memory_space=pltpu.SMEM)] + [in_vmem] * 4,
        out_specs=[in_vmem] * 2,
        out_shape=[
            jax.ShapeDtypeStruct((tokens, *ROW), jnp.bfloat16),
            jax.ShapeDtypeStruct((slots, *ROW), jnp.bfloat16),
        ],
        scratch_shapes=[
            pltpu.VMEM((tokens, D), jnp.bfloat16),
            pltpu.VMEM((tokens, D), jnp.bfloat16),
            pltpu.VMEM((tokens, *ROW), jnp.bfloat16),
        ],
        compiler_params=within(16),
        cost_estimate=pl.CostEstimate(
            flops=2 * tokens * D * D, bytes_accessed=2 * D * D, transcendentals=0
        ),
        name="middle",
    )(slot_token, on_chip(heads), on_chip(out_weight), on_chip(residual), gain)


def expert_kernel(tile_ref, gate_ref, up_ref, down_ref, out_ref, rows, hidden, result):
    count = tile_ref.shape[0]
    block = 512
    swap = swap_matrix()
    for one, two in pair_slices(count):
        rows[one, :], rows[two, :] = tiles_to_rows(tile_ref[one], tile_ref[two], swap)
    inputs = rows[...]
    for at in range(0, hidden.shape[1], block):
        columns = slice(at, at + block)
        gate = jnp.dot(inputs, gate_ref[:, columns], preferred_element_type=jnp.float32)
        up = jnp.dot(inputs, up_ref[:, columns], preferred_element_type=jnp.float32)
        hidden[:, columns] = (gate / (1.0 + jnp.exp(-gate)) * up).astype(jnp.bfloat16)
    acts = hidden[...]
    for at in range(0, D, block):
        columns = slice(at, at + block)
        result[:, columns] = jnp.dot(
            acts, down_ref[:, columns], preferred_element_type=jnp.float32
        ).astype(jnp.bfloat16)
    for one, two in pair_slices(count):
        out_ref[one], out_ref[two] = rows_to_tiles(result[one.start : two.stop, :], swap)


def expert_stage(tiles, gate, up, down):
    count = tiles.shape[0]
    width = gate.shape[1]
    in_vmem = pl.BlockSpec(memory_space=pltpu.VMEM)
    return pl.pallas_call(
        expert_kernel,
        in_specs=[in_vmem] * 4,
        out_specs=in_vmem,
        out_shape=jax.ShapeDtypeStruct((count, *ROW), jnp.bfloat16),
        scratch_shapes=[
            pltpu.VMEM((count, D), jnp.bfloat16),
            pltpu.VMEM((count, width), jnp.bfloat16),
            pltpu.VMEM((count, D), jnp.bfloat16),
        ],
        compiler_params=within(24),
        cost_estimate=pl.CostEstimate(
            flops=6 * count * D * width, bytes_accessed=6 * D * width, transcendentals=0
        ),
        name="experts",
    )(on_chip(tiles), on_chip(gate), on_chip(up), on_chip(down))


def combine_kernel(slot_ref, share_ref, mid_ref, back_ref, out_ref, tiles):
    tokens = mid_ref.shape[0]

    def token(index, carry):
        one = back_ref[slot_ref[2 * index]].astype(jnp.float32) * share_ref[2 * index]
        two = back_ref[slot_ref[2 * index + 1]].astype(jnp.float32) * share_ref[2 * index + 1]
        tiles[index] = (mid_ref[index].astype(jnp.float32) + (one + two)).astype(jnp.bfloat16)
        return carry

    lax.fori_loop(0, tokens, token, 0, unroll=16)
    swap = swap_matrix()
    for one, two in pair_slices(tokens):
        out_ref[one, :], out_ref[two, :] = tiles_to_rows(tiles[one], tiles[two], swap)


def combine_stage(slot, shares, mid, back):
    tokens = mid.shape[0]
    in_smem = pl.BlockSpec(memory_space=pltpu.SMEM)
    in_vmem = pl.BlockSpec(memory_space=pltpu.VMEM)
    return pl.pallas_call(
        combine_kernel,
        in_specs=[in_smem, in_smem, in_vmem, in_vmem],
        out_specs=in_vmem,
        out_shape=jax.ShapeDtypeStruct((tokens, D), jnp.bfloat16),
        scratch_shapes=[pltpu.VMEM((tokens, *ROW), jnp.bfloat16)],
        compiler_params=within(8),
        name="combine",
    )(slot, shares, on_chip(mid), on_chip(back))


def on_device(
    residual,
    query_maps,
    key_maps,
    value_rows,
    lambdas,
    head_gain,
    out_weight,
    ffn_gain,
    routes,
    route_weights,
    expert_gate,
    expert_up,
    expert_down,
):
    count_sp = lax.axis_size(SP)
    count_dp = lax.axis_size("dp")
    packed = pack_heads(query_maps[0], key_maps[0], value_rows[0])
    qkv = lax.all_to_all(packed, SP, split_axis=0, concat_axis=0, tiled=True)
    head = lax.axis_index(SP)
    lam_here = lax.dynamic_slice_in_dim(lambdas, head, 1)
    gain_here = lax.dynamic_slice_in_dim(head_gain, head * VD, VD)[None]
    attended = attention(lam_here, qkv, gain_here)
    returned = lax.all_to_all(attended, SP, split_axis=0, concat_axis=0, tiled=True)
    experts_all = count_sp * count_dp
    slot, slot_token = route_slots(routes[0].reshape(-1), experts_all)
    mid, sent = middle_stage(slot_token, returned, out_weight, residual[0], ffn_gain[None])
    arrived = lax.all_to_all(sent, SP_DP, split_axis=0, concat_axis=0, tiled=True)
    done = expert_stage(arrived, expert_gate[0], expert_up[0], expert_down[0])
    back = lax.all_to_all(done, SP_DP, split_axis=0, concat_axis=0, tiled=True)
    return combine_stage(slot, route_weights[0].reshape(-1), mid, back)[None]


def solution(mesh):
    finer = Mesh(mesh.devices.reshape(4, 4, mesh.shape["dp"]), ("sp_0", "sp_1", "dp"))
    placed = (
        P("dp", SP, None),
        P("dp", SP, None),
        P("dp", SP, None),
        P("dp", SP, None),
        P(),
        P(),
        P(),
        P(),
        P("dp", SP, None),
        P("dp", SP, None),
        P(SP_DP, None, None),
        P(SP_DP, None, None),
        P(SP_DP, None, None),
    )
    return jax.shard_map(
        on_device, mesh=finer, in_specs=placed, out_specs=P("dp", SP, None), check_vma=False
    )
```

```python
import math

import jax
import jax.numpy as jnp
from jax import lax
from jax.experimental import pallas as pl
from jax.experimental.pallas import tpu as pltpu
from jax.sharding import Mesh
from jax.sharding import PartitionSpec as P

D = 2048
HEADS = 16
HD = 64
VD = 128
SP = ("sp_0", "sp_1")
SP_DP = ("sp_0", "sp_1", "dp")


eps = 1e-06


def on_chip(value):
    return pltpu.with_memory_space_constraint(value, pltpu.VMEM)


def off_chip(value):
    return pltpu.with_memory_space_constraint(value, pltpu.HBM)


def within(mebibytes):
    return pltpu.CompilerParams(vmem_limit_bytes=mebibytes * 2**20)


EXP_SCALE = HD ** (-0.5) * math.log2(math.e)
LAST_DIMS = (((1,), (1,)), ((), ()))
ATT_BLOCKS = 2


def attention_kernel(
    lam_ref, qkv_ref, gain_ref, weight_hbm, routed_ref,
    out_ref, weight_ref, values_ref, scores_ref, sems,
):
    del routed_ref
    sources, _, tokens, width = qkv_ref.shape
    length = sources * tokens
    rows = ATT_BLOCKS * tokens
    steps = sources // ATT_BLOCKS
    fetch = pltpu.make_async_copy(weight_hbm, weight_ref, sems.at[0])
    fetch.start()
    values_ref[:, :VD] = qkv_ref[:, 2].reshape(length, width)
    values_ref[:, VD:] = jnp.ones((length, VD), jnp.bfloat16)

    def scores(step, slot):
        keys = qkv_ref[:, 1].reshape(length, width)
        query = qkv_ref[pl.ds(step * ATT_BLOCKS, ATT_BLOCKS), 0].reshape(rows, width)
        lane = lax.broadcasted_iota(jnp.int32, query.shape, 1)
        zero = jnp.zeros_like(query)
        both = jnp.concatenate(
            [jnp.where(lane < HD, query, zero), jnp.where(lane < HD, zero, query)], axis=0
        )
        scores_ref[slot] = lax.dot_general(
            both, keys, LAST_DIMS, preferred_element_type=jnp.float32
        )

    def attend(step, slot):
        score = scores_ref[slot]
        top = jnp.max(score, axis=-1, keepdims=True)
        weight = jnp.exp2((score - top) * EXP_SCALE).astype(jnp.bfloat16)
        summed = jnp.dot(weight, values_ref[...], preferred_element_type=jnp.float32)
        first, second = summed[:rows], summed[rows:]
        head_out = first[:, :VD] / first[:, VD:] - lam_ref[0] * (second[:, :VD] / second[:, VD:])
        normed = head_out * lax.rsqrt(jnp.mean(head_out * head_out, axis=-1, keepdims=True) + eps)
        at = pl.ds(step * ATT_BLOCKS, ATT_BLOCKS)
        out_ref[at] = (
            (normed * gain_ref[...] * 0.8).astype(jnp.bfloat16).reshape(ATT_BLOCKS, tokens, VD)
        )

    scores(0, 0)
    for step in range(1, steps):
        scores(step, step % 2)
        attend(step - 1, (step - 1) % 2)
    attend(steps - 1, (steps - 1) % 2)
    fetch.wait()


def attention(lam, qkv, gain, out_weight, routed):
    sources, _, tokens, width = qkv.shape
    length = sources * tokens
    in_vmem = pl.BlockSpec(memory_space=pltpu.VMEM)
    in_hbm = pl.BlockSpec(memory_space=pltpu.HBM)
    heads = (sources, tokens, VD)
    return pl.pallas_call(
        attention_kernel,
        in_specs=[pl.BlockSpec(memory_space=pltpu.SMEM), in_vmem, in_vmem, in_hbm]
        + [pl.BlockSpec(memory_space=pl.ANY)],
        out_specs=[in_vmem] * 2,
        out_shape=[
            jax.ShapeDtypeStruct(heads, jnp.bfloat16),
            pltpu.VMEM(out_weight.shape, jnp.bfloat16),
        ],
        scratch_shapes=[
            pltpu.VMEM((length, 2 * VD), jnp.bfloat16),
            pltpu.VMEM((2, 2 * ATT_BLOCKS * tokens, length), jnp.float32),
            pltpu.SemaphoreType.DMA((1,)),
        ],
        compiler_params=within(24),
        cost_estimate=pl.CostEstimate(
            flops=8 * length * length * VD,
            bytes_accessed=8 * length * VD,
            transcendentals=2 * length * length,
        ),
        name="attention",
    )(lam, on_chip(qkv), gain, off_chip(out_weight), routed)


ROW = (16, 128)
GROUP = 16
PAIR = 2 * GROUP
CAP = 4


def pack_kernel(query_ref, key_ref, value_ref, out_ref, rows, blocks, in_sems, out_sems):
    copies_in = [
        pltpu.make_async_copy(ref, rows.at[at], in_sems.at[at])
        for at, ref in enumerate((query_ref, key_ref, value_ref))
    ]
    copies_out = [
        pltpu.make_async_copy(blocks.at[:, at], out_ref.at[:, at], out_sems.at[at])
        for at in range(3)
    ]
    for copy in copies_in:
        copy.start()
    for at in range(3):
        copies_in[at].wait()
        for head in range(HEADS):
            blocks[head, at] = rows[at, :, head * VD : (head + 1) * VD]
        copies_out[at].start()
    for copy in copies_out:
        copy.wait()


def pack_heads(query, key, value):
    tokens = query.shape[0]
    packed = (HEADS, 3, tokens, VD)
    in_hbm = pl.BlockSpec(memory_space=pltpu.HBM)
    return pl.pallas_call(
        pack_kernel,
        in_specs=[in_hbm] * 3,
        out_specs=in_hbm,
        out_shape=pltpu.HBM(packed, jnp.bfloat16),
        scratch_shapes=[
            pltpu.VMEM((3, tokens, HEADS * VD), jnp.bfloat16),
            pltpu.VMEM(packed, jnp.bfloat16),
            pltpu.SemaphoreType.DMA((3,)),
            pltpu.SemaphoreType.DMA((3,)),
        ],
        compiler_params=within(8),
        name="pack_heads",
    )(*(off_chip(a) for a in (query, key, value)))


def route_kernel(routes_ref, shares_ref, slot_ref, token_ref, kept_ref, count_ref):
    experts = count_ref.shape[0]
    slots = token_ref.shape[0]

    def clear_count(index, carry):
        count_ref[index] = 0
        return carry

    def clear_token(index, carry):
        token_ref[index] = 0
        return carry

    def place(index, carry):
        expert = routes_ref[index]
        rank = count_ref[expert]
        count_ref[expert] = rank + 1
        slot = expert * CAP + rank
        slot_ref[index] = slot
        token_ref[slot] = index // 2
        kept_ref[index] = shares_ref[index]
        return carry

    lax.fori_loop(0, experts, clear_count, 0, unroll=8)
    lax.fori_loop(0, slots, clear_token, 0, unroll=8)
    lax.fori_loop(0, slot_ref.shape[0], place, 0)


def route_slots(flat_routes, flat_shares, experts):
    in_smem = pl.BlockSpec(memory_space=pltpu.SMEM)
    return pl.pallas_call(
        route_kernel,
        in_specs=[in_smem] * 2,
        out_specs=[in_smem] * 3,
        out_shape=[
            jax.ShapeDtypeStruct(flat_routes.shape, jnp.int32),
            jax.ShapeDtypeStruct((experts * CAP,), jnp.int32),
            jax.ShapeDtypeStruct(flat_shares.shape, jnp.float32),
        ],
        scratch_shapes=[pltpu.SMEM((experts,), jnp.int32)],
        compiler_params=within(1),
        name="route_slots",
    )(flat_routes, flat_shares)


def swap_matrix():
    size = GROUP * GROUP
    to = lax.broadcasted_iota(jnp.int32, (size, size), 0)
    at = lax.broadcasted_iota(jnp.int32, (size, size), 1)
    same = (to % GROUP) * GROUP + to // GROUP == at
    return jnp.where(same, 1.0, 0.0).astype(jnp.bfloat16)


def rows_to_tiles(rows, swap):
    halves = [
        jnp.concatenate(
            [rows[at : at + GROUP, 128 * j : 128 * (j + 1)] for j in range(16)], axis=0
        )
        for at in (0, GROUP)
    ]
    both = jnp.concatenate(halves, axis=1)
    swapped = jnp.dot(swap, both, preferred_element_type=jnp.float32).astype(jnp.bfloat16)
    return swapped[:, :128].reshape(GROUP, *ROW), swapped[:, 128:].reshape(GROUP, *ROW)


def tiles_to_rows(first, second, swap):
    size = GROUP * GROUP
    both = jnp.concatenate([first.reshape(size, 128), second.reshape(size, 128)], axis=1)
    swapped = jnp.dot(swap, both, preferred_element_type=jnp.float32).astype(jnp.bfloat16)
    return [
        jnp.concatenate(
            [swapped[GROUP * j : GROUP * (j + 1), at : at + 128] for j in range(16)], axis=1
        )
        for at in (0, 128)
    ]


def pair_slices(count):
    for at in range(0, count, PAIR):
        yield slice(at, at + GROUP), slice(at + GROUP, at + PAIR)


def middle_kernel(
    token_ref, heads_ref, weight_ref, residual_ref, gain_ref,
    mid_ref, sent_ref, heads_rows, middle, tiles,
):
    tokens = middle.shape[0]
    block = 512
    for head in range(HEADS):
        heads_rows[:, head * VD : (head + 1) * VD] = heads_ref[head]
    rows = heads_rows[...]
    squares = jnp.zeros((tokens, 128), jnp.float32)
    for at in range(0, D, block):
        columns = slice(at, at + block)
        projected = jnp.dot(rows, weight_ref[:, columns], preferred_element_type=jnp.float32)
        mid = (residual_ref[:, columns].astype(jnp.float32) + projected).astype(jnp.bfloat16)
        middle[:, columns] = mid
        wide = mid.astype(jnp.float32)
        wide = wide * wide
        for lane in range(0, block, 128):
            squares = squares + wide[:, lane : lane + 128]
    scale = lax.rsqrt(jnp.sum(squares, axis=-1, keepdims=True) / D + eps)
    swap = swap_matrix()
    for one, two in pair_slices(tokens):
        both = slice(one.start, two.stop)
        mid = middle[both, :]
        mid_ref[one], mid_ref[two] = rows_to_tiles(mid, swap)
        normed = mid.astype(jnp.float32) * scale[both] * gain_ref[...]
        tiles[one], tiles[two] = rows_to_tiles(normed.astype(jnp.bfloat16), swap)

    def gather(index, carry):
        sent_ref[index] = tiles[token_ref[index]]
        return carry

    lax.fori_loop(0, sent_ref.shape[0], gather, 0, unroll=16)


def middle_stage(slot_token, heads, out_weight, residual, gain):
    tokens = residual.shape[0]
    slots = slot_token.shape[0]
    in_vmem = pl.BlockSpec(memory_space=pltpu.VMEM)
    return pl.pallas_call(
        middle_kernel,
        in_specs=[pl.BlockSpec(memory_space=pltpu.SMEM)] + [in_vmem] * 4,
        out_specs=[in_vmem] * 2,
        out_shape=[
            jax.ShapeDtypeStruct((tokens, *ROW), jnp.bfloat16),
            jax.ShapeDtypeStruct((slots, *ROW), jnp.bfloat16),
        ],
        scratch_shapes=[
            pltpu.VMEM((tokens, D), jnp.bfloat16),
            pltpu.VMEM((tokens, D), jnp.bfloat16),
            pltpu.VMEM((tokens, *ROW), jnp.bfloat16),
        ],
        compiler_params=within(16),
        cost_estimate=pl.CostEstimate(
            flops=2 * tokens * D * D, bytes_accessed=2 * D * D, transcendentals=0
        ),
        name="middle",
    )(slot_token, on_chip(heads), on_chip(out_weight), on_chip(residual), gain)


def expert_kernel(tile_ref, gate_ref, up_ref, down_ref, out_ref, rows, hidden, result):
    count = tile_ref.shape[0]
    block = 256
    swap = swap_matrix()
    for one, two in pair_slices(count):
        rows[one, :], rows[two, :] = tiles_to_rows(tile_ref[one], tile_ref[two], swap)
    inputs = rows[...]
    for at in range(0, hidden.shape[1], block):
        columns = slice(at, at + block)
        gate = jnp.dot(inputs, gate_ref[:, columns], preferred_element_type=jnp.float32)
        up = jnp.dot(inputs, up_ref[:, columns], preferred_element_type=jnp.float32)
        hidden[:, columns] = (gate / (1.0 + jnp.exp(-gate)) * up).astype(jnp.bfloat16)
    acts = hidden[...]
    for at in range(0, D, 1024):
        columns = slice(at, at + 1024)
        result[:, columns] = jnp.dot(
            acts, down_ref[:, columns], preferred_element_type=jnp.float32
        ).astype(jnp.bfloat16)
    for one, two in pair_slices(count):
        out_ref[one], out_ref[two] = rows_to_tiles(result[one.start : two.stop, :], swap)


def expert_stage(tiles, gate, up, down):
    count = tiles.shape[0]
    width = gate.shape[1]
    in_vmem = pl.BlockSpec(memory_space=pltpu.VMEM)
    return pl.pallas_call(
        expert_kernel,
        in_specs=[in_vmem] * 4,
        out_specs=in_vmem,
        out_shape=jax.ShapeDtypeStruct((count, *ROW), jnp.bfloat16),
        scratch_shapes=[
            pltpu.VMEM((count, D), jnp.bfloat16),
            pltpu.VMEM((count, width), jnp.bfloat16),
            pltpu.VMEM((count, D), jnp.bfloat16),
        ],
        compiler_params=within(24),
        cost_estimate=pl.CostEstimate(
            flops=6 * count * D * width, bytes_accessed=6 * D * width, transcendentals=0
        ),
        name="experts",
    )(on_chip(tiles), on_chip(gate), on_chip(up), on_chip(down))


def combine_kernel(slot_ref, share_ref, mid_ref, back_ref, out_hbm, tiles, out_ref, sems):
    tokens = mid_ref.shape[0]

    def token(index, carry):
        one = back_ref[slot_ref[2 * index]].astype(jnp.float32) * share_ref[2 * index]
        two = back_ref[slot_ref[2 * index + 1]].astype(jnp.float32) * share_ref[2 * index + 1]
        tiles[index] = (mid_ref[index].astype(jnp.float32) + (one + two)).astype(jnp.bfloat16)
        return carry

    swap = swap_matrix()
    copies = []
    for one, two in pair_slices(tokens):
        lax.fori_loop(one.start, two.stop, token, 0, unroll=PAIR)
        out_ref[one, :], out_ref[two, :] = tiles_to_rows(tiles[one], tiles[two], swap)
        at = pl.ds(one.start, PAIR)
        copy = pltpu.make_async_copy(out_ref.at[at], out_hbm.at[at], sems.at[len(copies)])
        copy.start()
        copies.append(copy)
    for copy in copies:
        copy.wait()


def combine_stage(slot, shares, mid, back):
    tokens = mid.shape[0]
    in_smem = pl.BlockSpec(memory_space=pltpu.SMEM)
    in_vmem = pl.BlockSpec(memory_space=pltpu.VMEM)
    return pl.pallas_call(
        combine_kernel,
        in_specs=[in_smem, in_smem, in_vmem, in_vmem],
        out_specs=pl.BlockSpec(memory_space=pltpu.HBM),
        out_shape=pltpu.HBM((tokens, D), jnp.bfloat16),
        scratch_shapes=[
            pltpu.VMEM((tokens, *ROW), jnp.bfloat16),
            pltpu.VMEM((tokens, D), jnp.bfloat16),
            pltpu.SemaphoreType.DMA((tokens // PAIR,)),
        ],
        compiler_params=within(8),
        name="combine",
    )(slot, shares, on_chip(mid), on_chip(back))


def on_device(
    residual,
    query_maps,
    key_maps,
    value_rows,
    lambdas,
    head_gain,
    out_weight,
    ffn_gain,
    routes,
    route_weights,
    expert_gate,
    expert_up,
    expert_down,
):
    count_sp = lax.axis_size(SP)
    count_dp = lax.axis_size("dp")
    packed = pack_heads(query_maps[0], key_maps[0], value_rows[0])
    qkv = lax.all_to_all(packed, SP, split_axis=0, concat_axis=0, tiled=True)
    head = lax.axis_index(SP)
    lam_here = lax.dynamic_slice_in_dim(lambdas, head, 1)
    gain_here = lax.dynamic_slice_in_dim(head_gain, head * VD, VD)[None]
    experts_all = count_sp * count_dp
    slot, slot_token, shares = route_slots(
        routes[0].reshape(-1), route_weights[0].reshape(-1), experts_all
    )
    attended, weight_here = attention(lam_here, qkv, gain_here, out_weight, slot_token)
    returned = lax.all_to_all(attended, SP, split_axis=0, concat_axis=0, tiled=True)
    mid, sent = middle_stage(slot_token, returned, weight_here, residual[0], ffn_gain[None])
    arrived = lax.all_to_all(sent, SP_DP, split_axis=0, concat_axis=0, tiled=True)
    done = expert_stage(arrived, expert_gate[0], expert_up[0], expert_down[0])
    back = lax.all_to_all(done, SP_DP, split_axis=0, concat_axis=0, tiled=True)
    return combine_stage(slot, shares, mid, back)[None]


def solution(mesh):
    finer = Mesh(mesh.devices.reshape(4, 4, mesh.shape["dp"]), ("sp_0", "sp_1", "dp"))
    placed = (
        P("dp", SP, None),
        P("dp", SP, None),
        P("dp", SP, None),
        P("dp", SP, None),
        P(),
        P(),
        P(),
        P(),
        P("dp", SP, None),
        P("dp", SP, None),
        P(SP_DP, None, None),
        P(SP_DP, None, None),
        P(SP_DP, None, None),
    )
    return jax.shard_map(
        on_device, mesh=finer, in_specs=placed, out_specs=P("dp", SP, None), check_vma=False
    )
```

```python
import math

import jax
import jax.numpy as jnp
from jax import lax
from jax.experimental import pallas as pl
from jax.experimental.pallas import tpu as pltpu
from jax.sharding import Mesh
from jax.sharding import PartitionSpec as P

D = 2048
HEADS = 16
HD = 64
VD = 128
SP = ("sp_0", "sp_1")
SP_DP = ("sp_0", "sp_1", "dp")


eps = 1e-06


def on_chip(value):
    return pltpu.with_memory_space_constraint(value, pltpu.VMEM)


def off_chip(value):
    return pltpu.with_memory_space_constraint(value, pltpu.HBM)


def within(mebibytes):
    return pltpu.CompilerParams(vmem_limit_bytes=mebibytes * 2**20)


EXP_SCALE = HD ** (-0.5) * math.log2(math.e)
LAST_DIMS = (((1,), (1,)), ((), ()))
ATT_BLOCKS = 2


def attention_kernel(
    lam_ref, qkv_ref, gain_ref, weight_hbm, routes_ref,
    out_ref, weight_ref, slot_ref, token_ref, values_ref, scores_ref, count_ref, sems,
):
    head = lax.axis_index(SP)
    lam = lam_ref[head]
    gain = gain_ref[pl.ds(head, 1), :]
    experts = count_ref.shape[0]
    topk, tokens_here = routes_ref.shape
    routed = [(k, t) for k in range(topk) for t in range(tokens_here)]

    def clear_count(index, carry):
        count_ref[index] = 0
        return carry

    def clear_token(index, carry):
        token_ref[index] = 0
        return carry

    def route(places):
        for k, t in places:
            expert = routes_ref[k, t]
            rank = count_ref[expert]
            count_ref[expert] = rank + 1
            slot = expert * CAP + rank
            slot_ref[k, t] = slot
            token_ref[slot] = t

    sources, _, tokens, width = qkv_ref.shape
    length = sources * tokens
    rows = ATT_BLOCKS * tokens
    steps = sources // ATT_BLOCKS
    fetch = pltpu.make_async_copy(weight_hbm, weight_ref, sems.at[0])
    fetch.start()
    lax.fori_loop(0, experts, clear_count, 0, unroll=16)
    lax.fori_loop(0, token_ref.shape[0], clear_token, 0, unroll=16)
    values_ref[:, :VD] = qkv_ref[:, 2].reshape(length, width)
    values_ref[:, VD:] = jnp.ones((length, VD), jnp.bfloat16)

    def scores(step, slot):
        keys = qkv_ref[:, 1].reshape(length, width)
        query = qkv_ref[pl.ds(step * ATT_BLOCKS, ATT_BLOCKS), 0].reshape(rows, width)
        lane = lax.broadcasted_iota(jnp.int32, query.shape, 1)
        zero = jnp.zeros_like(query)
        both = jnp.concatenate(
            [jnp.where(lane < HD, query, zero), jnp.where(lane < HD, zero, query)], axis=0
        )
        scores_ref[slot] = lax.dot_general(
            both, keys, LAST_DIMS, preferred_element_type=jnp.float32
        )

    def attend(step, slot):
        score = scores_ref[slot]
        top = jnp.max(score, axis=-1, keepdims=True)
        weight = jnp.exp2((score - top) * EXP_SCALE).astype(jnp.bfloat16)
        summed = jnp.dot(weight, values_ref[...], preferred_element_type=jnp.float32)
        first, second = summed[:rows], summed[rows:]
        head_out = first[:, :VD] / first[:, VD:] - lam * (second[:, :VD] / second[:, VD:])
        normed = head_out * lax.rsqrt(jnp.mean(head_out * head_out, axis=-1, keepdims=True) + eps)
        at = pl.ds(step * ATT_BLOCKS, ATT_BLOCKS)
        out_ref[at] = (
            (normed * gain * 0.8).astype(jnp.bfloat16).reshape(ATT_BLOCKS, tokens, VD)
        )

    scores(0, 0)
    share = len(routed) // steps
    for step in range(1, steps):
        route(routed[(step - 1) * share : step * share])
        scores(step, step % 2)
        attend(step - 1, (step - 1) % 2)
    route(routed[(steps - 1) * share :])
    attend(steps - 1, (steps - 1) % 2)
    fetch.wait()


def attention(lam, qkv, gain, out_weight, routes, experts):
    sources, _, tokens, width = qkv.shape
    length = sources * tokens
    in_vmem = pl.BlockSpec(memory_space=pltpu.VMEM)
    in_hbm = pl.BlockSpec(memory_space=pltpu.HBM)
    in_smem = pl.BlockSpec(memory_space=pltpu.SMEM)
    heads = (sources, tokens, VD)
    return pl.pallas_call(
        attention_kernel,
        in_specs=[in_smem, in_vmem, in_vmem, in_hbm, in_smem],
        out_specs=[in_vmem, in_vmem, in_smem, in_smem],
        out_shape=[
            jax.ShapeDtypeStruct(heads, jnp.bfloat16),
            pltpu.VMEM(out_weight.shape, jnp.bfloat16),
            jax.ShapeDtypeStruct(routes.shape, jnp.int32),
            jax.ShapeDtypeStruct((experts * CAP,), jnp.int32),
        ],
        scratch_shapes=[
            pltpu.VMEM((length, 2 * VD), jnp.bfloat16),
            pltpu.VMEM((2, 2 * ATT_BLOCKS * tokens, length), jnp.float32),
            pltpu.SMEM((experts,), jnp.int32),
            pltpu.SemaphoreType.DMA((1,)),
        ],
        compiler_params=within(24),
        cost_estimate=pl.CostEstimate(
            flops=8 * length * length * VD,
            bytes_accessed=8 * length * VD,
            transcendentals=2 * length * length,
        ),
        name="attention",
    )(lam, on_chip(qkv), gain, off_chip(out_weight), routes)


ROW = (16, 128)
GROUP = 16
PAIR = 2 * GROUP
CAP = 4


def pack_kernel(query_ref, key_ref, value_ref, out_ref, rows, sems):
    copies = [
        pltpu.make_async_copy(ref, rows.at[at], sems.at[at])
        for at, ref in enumerate((query_ref, key_ref, value_ref))
    ]
    for copy in copies:
        copy.start()
    for at in range(3):
        copies[at].wait()
        for head in range(HEADS):
            out_ref[head, at] = rows[at, :, head * VD : (head + 1) * VD]


def pack_heads(query, key, value):
    tokens = query.shape[0]
    in_hbm = pl.BlockSpec(memory_space=pltpu.HBM)
    return pl.pallas_call(
        pack_kernel,
        in_specs=[in_hbm] * 3,
        out_specs=pl.BlockSpec(memory_space=pltpu.VMEM),
        out_shape=jax.ShapeDtypeStruct((HEADS, 3, tokens, VD), jnp.bfloat16),
        scratch_shapes=[
            pltpu.VMEM((3, tokens, HEADS * VD), jnp.bfloat16),
            pltpu.SemaphoreType.DMA((3,)),
        ],
        compiler_params=within(8),
        name="pack_heads",
    )(*(off_chip(a) for a in (query, key, value)))


def swap_matrix():
    size = GROUP * GROUP
    to = lax.broadcasted_iota(jnp.int32, (size, size), 0)
    at = lax.broadcasted_iota(jnp.int32, (size, size), 1)
    same = (to % GROUP) * GROUP + to // GROUP == at
    return jnp.where(same, 1.0, 0.0).astype(jnp.bfloat16)


def rows_to_tiles(rows, swap):
    halves = [
        jnp.concatenate(
            [rows[at : at + GROUP, 128 * j : 128 * (j + 1)] for j in range(16)], axis=0
        )
        for at in (0, GROUP)
    ]
    both = jnp.concatenate(halves, axis=1)
    swapped = jnp.dot(swap, both, preferred_element_type=jnp.float32).astype(jnp.bfloat16)
    return swapped[:, :128].reshape(GROUP, *ROW), swapped[:, 128:].reshape(GROUP, *ROW)


def tiles_to_rows(first, second, swap):
    size = GROUP * GROUP
    both = jnp.concatenate([first.reshape(size, 128), second.reshape(size, 128)], axis=1)
    swapped = jnp.dot(swap, both, preferred_element_type=jnp.float32).astype(jnp.bfloat16)
    return [
        jnp.concatenate(
            [swapped[GROUP * j : GROUP * (j + 1), at : at + 128] for j in range(16)], axis=1
        )
        for at in (0, 128)
    ]


def pair_slices(count):
    for at in range(0, count, PAIR):
        yield slice(at, at + GROUP), slice(at + GROUP, at + PAIR)


def middle_kernel(
    token_ref, heads_ref, weight_ref, residual_ref, gain_ref,
    mid_ref, sent_ref, heads_rows, middle, tiles,
):
    tokens = middle.shape[0]
    block = 512
    for head in range(HEADS):
        heads_rows[:, head * VD : (head + 1) * VD] = heads_ref[head]
    rows = heads_rows[...]
    squares = jnp.zeros((tokens, 128), jnp.float32)
    for at in range(0, D, block):
        columns = slice(at, at + block)
        projected = jnp.dot(rows, weight_ref[:, columns], preferred_element_type=jnp.float32)
        mid = (residual_ref[:, columns].astype(jnp.float32) + projected).astype(jnp.bfloat16)
        middle[:, columns] = mid
        wide = mid.astype(jnp.float32)
        wide = wide * wide
        for lane in range(0, block, 128):
            squares = squares + wide[:, lane : lane + 128]
    scale = lax.rsqrt(jnp.sum(squares, axis=-1, keepdims=True) / D + eps)
    swap = swap_matrix()
    for one, two in pair_slices(tokens):
        both = slice(one.start, two.stop)
        mid = middle[both, :]
        mid_ref[one], mid_ref[two] = rows_to_tiles(mid, swap)
        normed = mid.astype(jnp.float32) * scale[both] * gain_ref[...]
        tiles[one], tiles[two] = rows_to_tiles(normed.astype(jnp.bfloat16), swap)

    def gather(index, carry):
        sent_ref[index] = tiles[token_ref[index]]
        return carry

    lax.fori_loop(0, sent_ref.shape[0], gather, 0, unroll=16)


def middle_stage(slot_token, heads, out_weight, residual, gain):
    tokens = residual.shape[0]
    slots = slot_token.shape[0]
    in_vmem = pl.BlockSpec(memory_space=pltpu.VMEM)
    return pl.pallas_call(
        middle_kernel,
        in_specs=[pl.BlockSpec(memory_space=pltpu.SMEM)] + [in_vmem] * 4,
        out_specs=[in_vmem] * 2,
        out_shape=[
            jax.ShapeDtypeStruct((tokens, *ROW), jnp.bfloat16),
            jax.ShapeDtypeStruct((slots, *ROW), jnp.bfloat16),
        ],
        scratch_shapes=[
            pltpu.VMEM((tokens, D), jnp.bfloat16),
            pltpu.VMEM((tokens, D), jnp.bfloat16),
            pltpu.VMEM((tokens, *ROW), jnp.bfloat16),
        ],
        compiler_params=within(16),
        cost_estimate=pl.CostEstimate(
            flops=2 * tokens * D * D, bytes_accessed=2 * D * D, transcendentals=0
        ),
        name="middle",
    )(slot_token, on_chip(heads), on_chip(out_weight), on_chip(residual), gain)


def expert_kernel(tile_ref, gate_ref, up_ref, down_ref, out_ref, rows, hidden, result):
    count = tile_ref.shape[0]
    block = 256
    swap = swap_matrix()
    for one, two in pair_slices(count):
        rows[one, :], rows[two, :] = tiles_to_rows(tile_ref[one], tile_ref[two], swap)
    inputs = rows[...]
    for at in range(0, hidden.shape[1], block):
        columns = slice(at, at + block)
        gate = jnp.dot(inputs, gate_ref[:, columns], preferred_element_type=jnp.float32)
        up = jnp.dot(inputs, up_ref[:, columns], preferred_element_type=jnp.float32)
        hidden[:, columns] = (gate / (1.0 + jnp.exp(-gate)) * up).astype(jnp.bfloat16)
    acts = hidden[...]
    for at in range(0, D, 1024):
        columns = slice(at, at + 1024)
        result[:, columns] = jnp.dot(
            acts, down_ref[:, columns], preferred_element_type=jnp.float32
        ).astype(jnp.bfloat16)
    for one, two in pair_slices(count):
        out_ref[one], out_ref[two] = rows_to_tiles(result[one.start : two.stop, :], swap)


def expert_stage(tiles, gate, up, down):
    count = tiles.shape[0]
    width = gate.shape[1]
    in_vmem = pl.BlockSpec(memory_space=pltpu.VMEM)
    return pl.pallas_call(
        expert_kernel,
        in_specs=[in_vmem] * 4,
        out_specs=in_vmem,
        out_shape=jax.ShapeDtypeStruct((count, *ROW), jnp.bfloat16),
        scratch_shapes=[
            pltpu.VMEM((count, D), jnp.bfloat16),
            pltpu.VMEM((count, width), jnp.bfloat16),
            pltpu.VMEM((count, D), jnp.bfloat16),
        ],
        compiler_params=within(24),
        cost_estimate=pl.CostEstimate(
            flops=6 * count * D * width, bytes_accessed=6 * D * width, transcendentals=0
        ),
        name="experts",
    )(on_chip(tiles), on_chip(gate), on_chip(up), on_chip(down))


def combine_kernel(slot_ref, share_ref, mid_ref, back_ref, out_hbm, tiles, out_ref, sems):
    tokens = mid_ref.shape[0]

    def token(index, carry):
        one = back_ref[slot_ref[0, index]].astype(jnp.float32) * share_ref[0, index]
        two = back_ref[slot_ref[1, index]].astype(jnp.float32) * share_ref[1, index]
        tiles[index] = (mid_ref[index].astype(jnp.float32) + (one + two)).astype(jnp.bfloat16)
        return carry

    swap = swap_matrix()
    copies = []
    for one, two in pair_slices(tokens):
        lax.fori_loop(one.start, two.stop, token, 0, unroll=PAIR)
        out_ref[one, :], out_ref[two, :] = tiles_to_rows(tiles[one], tiles[two], swap)
        at = pl.ds(one.start, PAIR)
        copy = pltpu.make_async_copy(out_ref.at[at], out_hbm.at[at], sems.at[len(copies)])
        copy.start()
        copies.append(copy)
    for copy in copies:
        copy.wait()


def combine_stage(slot, shares, mid, back):
    tokens = mid.shape[0]
    in_smem = pl.BlockSpec(memory_space=pltpu.SMEM)
    in_vmem = pl.BlockSpec(memory_space=pltpu.VMEM)
    return pl.pallas_call(
        combine_kernel,
        in_specs=[in_smem, in_smem, in_vmem, in_vmem],
        out_specs=pl.BlockSpec(memory_space=pltpu.HBM),
        out_shape=pltpu.HBM((tokens, D), jnp.bfloat16),
        scratch_shapes=[
            pltpu.VMEM((tokens, *ROW), jnp.bfloat16),
            pltpu.VMEM((tokens, D), jnp.bfloat16),
            pltpu.SemaphoreType.DMA((tokens // PAIR,)),
        ],
        compiler_params=within(8),
        name="combine",
    )(slot, shares, on_chip(mid), on_chip(back))


def on_device(
    residual,
    query_maps,
    key_maps,
    value_rows,
    lambdas,
    head_gain,
    out_weight,
    ffn_gain,
    routes,
    route_weights,
    expert_gate,
    expert_up,
    expert_down,
):
    count_sp = lax.axis_size(SP)
    count_dp = lax.axis_size("dp")
    packed = pack_heads(query_maps[0], key_maps[0], value_rows[0])
    qkv = lax.all_to_all(packed, SP, split_axis=0, concat_axis=0, tiled=True)
    experts_all = count_sp * count_dp
    attended, weight_here, slot, slot_token = attention(
        lambdas, qkv, head_gain.reshape(HEADS, VD), out_weight, routes[0].T, experts_all
    )
    returned = lax.all_to_all(attended, SP, split_axis=0, concat_axis=0, tiled=True)
    mid, sent = middle_stage(slot_token, returned, weight_here, residual[0], ffn_gain[None])
    arrived = lax.all_to_all(sent, SP_DP, split_axis=0, concat_axis=0, tiled=True)
    done = expert_stage(arrived, expert_gate[0], expert_up[0], expert_down[0])
    back = lax.all_to_all(done, SP_DP, split_axis=0, concat_axis=0, tiled=True)
    return combine_stage(slot, route_weights[0].T, mid, back)[None]


def solution(mesh):
    finer = Mesh(mesh.devices.reshape(4, 4, mesh.shape["dp"]), ("sp_0", "sp_1", "dp"))
    placed = (
        P("dp", SP, None),
        P("dp", SP, None),
        P("dp", SP, None),
        P("dp", SP, None),
        P(),
        P(),
        P(),
        P(),
        P("dp", SP, None),
        P("dp", SP, None),
        P(SP_DP, None, None),
        P(SP_DP, None, None),
        P(SP_DP, None, None),
    )
    return jax.shard_map(
        on_device, mesh=finer, in_specs=placed, out_specs=P("dp", SP, None), check_vma=False
    )
```

```python
import math

import jax
import jax.numpy as jnp
from jax import lax
from jax.experimental import pallas as pl
from jax.experimental.pallas import tpu as pltpu
from jax.sharding import Mesh
from jax.sharding import PartitionSpec as P

D = 2048
HEADS = 16
HD = 64
VD = 128
SP = ("sp_0", "sp_1")
SP_DP = ("sp_0", "sp_1", "dp")


eps = 1e-06


def on_chip(value):
    return pltpu.with_memory_space_constraint(value, pltpu.VMEM)


def off_chip(value):
    return pltpu.with_memory_space_constraint(value, pltpu.HBM)


def within(mebibytes):
    return pltpu.CompilerParams(vmem_limit_bytes=mebibytes * 2**20)


EXP_SCALE = HD ** (-0.5) * math.log2(math.e)
LAST_DIMS = (((1,), (1,)), ((), ()))
ATT_BLOCKS = 2


def attention_kernel(
    lam_ref, qkv_ref, gain_ref, weight_hbm, routes_ref,
    out_ref, weight_ref, slot_ref, token_ref, values_ref, scores_ref, count_ref, sems,
):
    head = lax.axis_index(SP)
    lam = lam_ref[head]
    gain = gain_ref[pl.ds(head, 1), :]
    experts = count_ref.shape[0]
    topk, tokens_here = routes_ref.shape
    routed = [(k, t) for k in range(topk) for t in range(tokens_here)]

    def route(places):
        for k, t in places:
            expert = routes_ref[k, t]
            rank = count_ref[expert]
            count_ref[expert] = rank + 1
            slot = expert * CAP + rank
            slot_ref[k, t] = slot
            token_ref[slot] = t

    sources, _, tokens, width = qkv_ref.shape
    length = sources * tokens
    rows = ATT_BLOCKS * tokens
    steps = sources // ATT_BLOCKS
    fetch = pltpu.make_async_copy(weight_hbm, weight_ref, sems.at[0])
    fetch.start()
    for index in range(experts):
        count_ref[index] = 0
    for index in range(token_ref.shape[0]):
        token_ref[index] = 0
    values_ref[:, :VD] = qkv_ref[:, 2].reshape(length, width)
    values_ref[:, VD:] = jnp.ones((length, VD), jnp.bfloat16)

    def scores(step, slot):
        keys = qkv_ref[:, 1].reshape(length, width)
        query = qkv_ref[pl.ds(step * ATT_BLOCKS, ATT_BLOCKS), 0].reshape(rows, width)
        lane = lax.broadcasted_iota(jnp.int32, query.shape, 1)
        zero = jnp.zeros_like(query)
        both = jnp.concatenate(
            [jnp.where(lane < HD, query, zero), jnp.where(lane < HD, zero, query)], axis=0
        )
        scores_ref[slot] = lax.dot_general(
            both, keys, LAST_DIMS, preferred_element_type=jnp.float32
        )

    def attend(step, slot):
        score = scores_ref[slot]
        top = jnp.max(score, axis=-1, keepdims=True)
        weight = jnp.exp2((score - top) * EXP_SCALE).astype(jnp.bfloat16)
        summed = jnp.dot(weight, values_ref[...], preferred_element_type=jnp.float32)
        first, second = summed[:rows], summed[rows:]
        head_out = first[:, :VD] / first[:, VD:] - lam * (second[:, :VD] / second[:, VD:])
        normed = head_out * lax.rsqrt(jnp.mean(head_out * head_out, axis=-1, keepdims=True) + eps)
        at = pl.ds(step * ATT_BLOCKS, ATT_BLOCKS)
        out_ref[at] = (
            (normed * gain * 0.8).astype(jnp.bfloat16).reshape(ATT_BLOCKS, tokens, VD)
        )

    scores(0, 0)
    share = len(routed) // steps
    for step in range(1, steps):
        route(routed[(step - 1) * share : step * share])
        scores(step, step % 2)
        attend(step - 1, (step - 1) % 2)
    route(routed[(steps - 1) * share :])
    attend(steps - 1, (steps - 1) % 2)
    fetch.wait()


def attention(lam, qkv, gain, out_weight, routes, experts):
    sources, _, tokens, width = qkv.shape
    length = sources * tokens
    in_vmem = pl.BlockSpec(memory_space=pltpu.VMEM)
    in_hbm = pl.BlockSpec(memory_space=pltpu.HBM)
    in_smem = pl.BlockSpec(memory_space=pltpu.SMEM)
    heads = (sources, tokens, VD)
    return pl.pallas_call(
        attention_kernel,
        in_specs=[in_smem, in_vmem, in_vmem, in_hbm, in_smem],
        out_specs=[in_vmem, in_vmem, in_smem, in_smem],
        out_shape=[
            jax.ShapeDtypeStruct(heads, jnp.bfloat16),
            pltpu.VMEM(out_weight.shape, jnp.bfloat16),
            jax.ShapeDtypeStruct(routes.shape, jnp.int32),
            jax.ShapeDtypeStruct((experts * CAP,), jnp.int32),
        ],
        scratch_shapes=[
            pltpu.VMEM((length, 2 * VD), jnp.bfloat16),
            pltpu.VMEM((2, 2 * ATT_BLOCKS * tokens, length), jnp.float32),
            pltpu.SMEM((experts,), jnp.int32),
            pltpu.SemaphoreType.DMA((1,)),
        ],
        compiler_params=within(24),
        cost_estimate=pl.CostEstimate(
            flops=8 * length * length * VD,
            bytes_accessed=8 * length * VD,
            transcendentals=2 * length * length,
        ),
        name="attention",
    )(lam, on_chip(qkv), gain, off_chip(out_weight), routes)


ROW = (16, 128)
GROUP = 16
PAIR = 2 * GROUP
CAP = 4


def pack_kernel(query_ref, key_ref, value_ref, out_ref, rows, sems):
    copies = [
        pltpu.make_async_copy(ref, rows.at[at], sems.at[at])
        for at, ref in enumerate((query_ref, key_ref, value_ref))
    ]
    for copy in copies:
        copy.start()
    for at in range(3):
        copies[at].wait()
        for head in range(HEADS):
            out_ref[head, at] = rows[at, :, head * VD : (head + 1) * VD]


def pack_heads(query, key, value):
    tokens = query.shape[0]
    in_hbm = pl.BlockSpec(memory_space=pltpu.HBM)
    return pl.pallas_call(
        pack_kernel,
        in_specs=[in_hbm] * 3,
        out_specs=pl.BlockSpec(memory_space=pltpu.VMEM),
        out_shape=jax.ShapeDtypeStruct((HEADS, 3, tokens, VD), jnp.bfloat16),
        scratch_shapes=[
            pltpu.VMEM((3, tokens, HEADS * VD), jnp.bfloat16),
            pltpu.SemaphoreType.DMA((3,)),
        ],
        compiler_params=within(8),
        name="pack_heads",
    )(*(off_chip(a) for a in (query, key, value)))


def swap_matrix():
    size = GROUP * GROUP
    to = lax.broadcasted_iota(jnp.int32, (size, size), 0)
    at = lax.broadcasted_iota(jnp.int32, (size, size), 1)
    same = (to % GROUP) * GROUP + to // GROUP == at
    return jnp.where(same, 1.0, 0.0).astype(jnp.bfloat16)


def rows_to_tiles(rows, swap):
    halves = [
        jnp.concatenate(
            [rows[at : at + GROUP, 128 * j : 128 * (j + 1)] for j in range(16)], axis=0
        )
        for at in (0, GROUP)
    ]
    both = jnp.concatenate(halves, axis=1)
    swapped = jnp.dot(swap, both, preferred_element_type=jnp.float32).astype(jnp.bfloat16)
    return swapped[:, :128].reshape(GROUP, *ROW), swapped[:, 128:].reshape(GROUP, *ROW)


def tiles_to_rows(first, second, swap):
    size = GROUP * GROUP
    both = jnp.concatenate([first.reshape(size, 128), second.reshape(size, 128)], axis=1)
    swapped = jnp.dot(swap, both, preferred_element_type=jnp.float32).astype(jnp.bfloat16)
    return [
        jnp.concatenate(
            [swapped[GROUP * j : GROUP * (j + 1), at : at + 128] for j in range(16)], axis=1
        )
        for at in (0, 128)
    ]


def pair_slices(count):
    for at in range(0, count, PAIR):
        yield slice(at, at + GROUP), slice(at + GROUP, at + PAIR)


def middle_kernel(
    token_ref, heads_ref, weight_ref, residual_ref, gain_ref,
    mid_ref, sent_ref, heads_rows, middle, tiles,
):
    tokens = middle.shape[0]
    block = 512
    for head in range(HEADS):
        heads_rows[:, head * VD : (head + 1) * VD] = heads_ref[head]
    rows = heads_rows[...]
    squares = jnp.zeros((tokens, 128), jnp.float32)
    for at in range(0, D, block):
        columns = slice(at, at + block)
        projected = jnp.dot(rows, weight_ref[:, columns], preferred_element_type=jnp.float32)
        mid = (residual_ref[:, columns].astype(jnp.float32) + projected).astype(jnp.bfloat16)
        middle[:, columns] = mid
        wide = mid.astype(jnp.float32)
        wide = wide * wide
        for lane in range(0, block, 128):
            squares = squares + wide[:, lane : lane + 128]
    scale = lax.rsqrt(jnp.sum(squares, axis=-1, keepdims=True) / D + eps)
    swap = swap_matrix()
    for one, two in pair_slices(tokens):
        both = slice(one.start, two.stop)
        normed = middle[both, :].astype(jnp.float32) * scale[both] * gain_ref[...]
        tiles[one], tiles[two] = rows_to_tiles(normed.astype(jnp.bfloat16), swap)

    for index in range(sent_ref.shape[0]):
        sent_ref[index] = tiles[token_ref[index]]
    for one, two in pair_slices(tokens):
        mid_ref[one], mid_ref[two] = rows_to_tiles(middle[one.start : two.stop, :], swap)


def middle_stage(slot_token, heads, out_weight, residual, gain):
    tokens = residual.shape[0]
    slots = slot_token.shape[0]
    in_vmem = pl.BlockSpec(memory_space=pltpu.VMEM)
    return pl.pallas_call(
        middle_kernel,
        in_specs=[pl.BlockSpec(memory_space=pltpu.SMEM)] + [in_vmem] * 4,
        out_specs=[in_vmem] * 2,
        out_shape=[
            jax.ShapeDtypeStruct((tokens, *ROW), jnp.bfloat16),
            jax.ShapeDtypeStruct((slots, *ROW), jnp.bfloat16),
        ],
        scratch_shapes=[
            pltpu.VMEM((tokens, D), jnp.bfloat16),
            pltpu.VMEM((tokens, D), jnp.bfloat16),
            pltpu.VMEM((tokens, *ROW), jnp.bfloat16),
        ],
        compiler_params=within(16),
        cost_estimate=pl.CostEstimate(
            flops=2 * tokens * D * D, bytes_accessed=2 * D * D, transcendentals=0
        ),
        name="middle",
    )(slot_token, on_chip(heads), on_chip(out_weight), on_chip(residual), gain)


def expert_kernel(tile_ref, gate_ref, up_ref, down_ref, out_ref, rows, hidden, result):
    count = tile_ref.shape[0]
    block = 256
    swap = swap_matrix()
    for one, two in pair_slices(count):
        rows[one, :], rows[two, :] = tiles_to_rows(tile_ref[one], tile_ref[two], swap)
    inputs = rows[...]
    for at in range(0, hidden.shape[1], block):
        columns = slice(at, at + block)
        gate = jnp.dot(inputs, gate_ref[:, columns], preferred_element_type=jnp.float32)
        up = jnp.dot(inputs, up_ref[:, columns], preferred_element_type=jnp.float32)
        hidden[:, columns] = (gate / (1.0 + jnp.exp(-gate)) * up).astype(jnp.bfloat16)
    acts = hidden[...]
    for at in range(0, D, 1024):
        columns = slice(at, at + 1024)
        result[:, columns] = jnp.dot(
            acts, down_ref[:, columns], preferred_element_type=jnp.float32
        ).astype(jnp.bfloat16)
    for one, two in pair_slices(count):
        out_ref[one], out_ref[two] = rows_to_tiles(result[one.start : two.stop, :], swap)


def expert_stage(tiles, gate, up, down):
    count = tiles.shape[0]
    width = gate.shape[1]
    in_vmem = pl.BlockSpec(memory_space=pltpu.VMEM)
    return pl.pallas_call(
        expert_kernel,
        in_specs=[in_vmem] * 4,
        out_specs=in_vmem,
        out_shape=jax.ShapeDtypeStruct((count, *ROW), jnp.bfloat16),
        scratch_shapes=[
            pltpu.VMEM((count, D), jnp.bfloat16),
            pltpu.VMEM((count, width), jnp.bfloat16),
            pltpu.VMEM((count, D), jnp.bfloat16),
        ],
        compiler_params=within(24),
        cost_estimate=pl.CostEstimate(
            flops=6 * count * D * width, bytes_accessed=6 * D * width, transcendentals=0
        ),
        name="experts",
    )(on_chip(tiles), on_chip(gate), on_chip(up), on_chip(down))


def combine_kernel(slot_ref, share_ref, mid_ref, back_ref, out_hbm, tiles, out_ref, sems):
    tokens = mid_ref.shape[0]

    def token(index, carry):
        one = back_ref[slot_ref[0, index]].astype(jnp.float32) * share_ref[0, index]
        two = back_ref[slot_ref[1, index]].astype(jnp.float32) * share_ref[1, index]
        tiles[index] = (mid_ref[index].astype(jnp.float32) + (one + two)).astype(jnp.bfloat16)
        return carry

    swap = swap_matrix()
    copies = []
    for one, two in pair_slices(tokens):
        lax.fori_loop(one.start, two.stop, token, 0, unroll=PAIR)
        out_ref[one, :], out_ref[two, :] = tiles_to_rows(tiles[one], tiles[two], swap)
        at = pl.ds(one.start, PAIR)
        copy = pltpu.make_async_copy(out_ref.at[at], out_hbm.at[at], sems.at[len(copies)])
        copy.start()
        copies.append(copy)
    for copy in copies:
        copy.wait()


def combine_stage(slot, shares, mid, back):
    tokens = mid.shape[0]
    in_smem = pl.BlockSpec(memory_space=pltpu.SMEM)
    in_vmem = pl.BlockSpec(memory_space=pltpu.VMEM)
    return pl.pallas_call(
        combine_kernel,
        in_specs=[in_smem, in_smem, in_vmem, in_vmem],
        out_specs=pl.BlockSpec(memory_space=pltpu.HBM),
        out_shape=pltpu.HBM((tokens, D), jnp.bfloat16),
        scratch_shapes=[
            pltpu.VMEM((tokens, *ROW), jnp.bfloat16),
            pltpu.VMEM((tokens, D), jnp.bfloat16),
            pltpu.SemaphoreType.DMA((tokens // PAIR,)),
        ],
        compiler_params=within(8),
        name="combine",
    )(slot, shares, on_chip(mid), on_chip(back))


def on_device(
    residual,
    query_maps,
    key_maps,
    value_rows,
    lambdas,
    head_gain,
    out_weight,
    ffn_gain,
    routes,
    route_weights,
    expert_gate,
    expert_up,
    expert_down,
):
    count_sp = lax.axis_size(SP)
    count_dp = lax.axis_size("dp")
    packed = pack_heads(query_maps[0], key_maps[0], value_rows[0])
    qkv = lax.all_to_all(packed, SP, split_axis=0, concat_axis=0, tiled=True)
    experts_all = count_sp * count_dp
    attended, weight_here, slot, slot_token = attention(
        lambdas, qkv, head_gain.reshape(HEADS, VD), out_weight, routes[0].T, experts_all
    )
    returned = lax.all_to_all(attended, SP, split_axis=0, concat_axis=0, tiled=True)
    mid, sent = middle_stage(slot_token, returned, weight_here, residual[0], ffn_gain[None])
    arrived = lax.all_to_all(sent, SP_DP, split_axis=0, concat_axis=0, tiled=True)
    done = expert_stage(arrived, expert_gate[0], expert_up[0], expert_down[0])
    back = lax.all_to_all(done, SP_DP, split_axis=0, concat_axis=0, tiled=True)
    return combine_stage(slot, route_weights[0].T, mid, back)[None]


def solution(mesh):
    finer = Mesh(mesh.devices.reshape(4, 4, mesh.shape["dp"]), ("sp_0", "sp_1", "dp"))
    placed = (
        P("dp", SP, None),
        P("dp", SP, None),
        P("dp", SP, None),
        P("dp", SP, None),
        P(),
        P(),
        P(),
        P(),
        P("dp", SP, None),
        P("dp", SP, None),
        P(SP_DP, None, None),
        P(SP_DP, None, None),
        P(SP_DP, None, None),
    )
    return jax.shard_map(
        on_device, mesh=finer, in_specs=placed, out_specs=P("dp", SP, None), check_vma=False
    )
```

```python
import math

import jax
import jax.numpy as jnp
from jax import lax
from jax.experimental import pallas as pl
from jax.experimental.pallas import tpu as pltpu
from jax.sharding import Mesh
from jax.sharding import PartitionSpec as P

D = 2048
HEADS = 16
HD = 64
VD = 128
SP = ("sp_0", "sp_1")
SP_DP = ("sp_0", "sp_1", "dp")


eps = 1e-06


def on_chip(value):
    return pltpu.with_memory_space_constraint(value, pltpu.VMEM)


def off_chip(value):
    return pltpu.with_memory_space_constraint(value, pltpu.HBM)


def within(mebibytes):
    return pltpu.CompilerParams(vmem_limit_bytes=mebibytes * 2**20)


EXP_SCALE = HD ** (-0.5) * math.log2(math.e)
LAST_DIMS = (((1,), (1,)), ((), ()))
ATT_BLOCKS = 2


def route_rows(routes_ref, slot_ref, token_ref):
    experts = token_ref.shape[1]
    topk, tokens = routes_ref.shape
    expert_at = lax.broadcasted_iota(jnp.int32, (experts, tokens), 0)
    square = (tokens, tokens)
    earlier = lax.broadcasted_iota(jnp.int32, square, 0) < lax.broadcasted_iota(
        jnp.int32, square, 1
    )
    earlier = jnp.where(earlier, 1.0, 0.0).astype(jnp.bfloat16)
    taken = jnp.zeros((experts, 1), jnp.float32)
    ranked = [jnp.zeros((experts, tokens), jnp.float32) for _ in range(CAP)]
    for k in range(topk):
        here = jnp.where(expert_at == routes_ref[k : k + 1, :], 1.0, 0.0)
        before = taken + jnp.dot(
            here.astype(jnp.bfloat16), earlier, preferred_element_type=jnp.float32
        )
        slot = here * (CAP * expert_at.astype(jnp.float32) + before)
        slot_ref[k : k + 1, :] = jnp.sum(slot, axis=0, keepdims=True).astype(jnp.int32)
        taken = taken + jnp.sum(here, axis=1, keepdims=True)
        for rank in range(CAP):
            ranked[rank] = ranked[rank] + jnp.where(before == rank, here, 0.0)
    token_at = lax.broadcasted_iota(jnp.int32, (16, tokens), 1).astype(jnp.float32)
    for rank in range(CAP):
        of_slot = lax.dot_general(
            token_at.astype(jnp.bfloat16),
            ranked[rank].astype(jnp.bfloat16),
            LAST_DIMS,
            preferred_element_type=jnp.float32,
        )
        token_ref[rank : rank + 1, :] = of_slot[:1].astype(jnp.int32)


def attention_kernel(
    lam_ref, qkv_ref, gain_ref, weight_hbm, routes_ref,
    out_ref, weight_ref, slot_ref, token_ref, values_ref, scores_ref, sems,
):
    head = lax.axis_index(SP)
    lam = lam_ref[head]
    gain = gain_ref[pl.ds(head, 1), :]
    sources, _, tokens, width = qkv_ref.shape
    length = sources * tokens
    rows = ATT_BLOCKS * tokens
    steps = sources // ATT_BLOCKS
    fetch = pltpu.make_async_copy(weight_hbm, weight_ref, sems.at[0])
    fetch.start()
    route_rows(routes_ref, slot_ref, token_ref)
    values_ref[:, :VD] = qkv_ref[:, 2].reshape(length, width)
    values_ref[:, VD:] = jnp.ones((length, VD), jnp.bfloat16)

    def scores(step, slot):
        keys = qkv_ref[:, 1].reshape(length, width)
        query = qkv_ref[pl.ds(step * ATT_BLOCKS, ATT_BLOCKS), 0].reshape(rows, width)
        lane = lax.broadcasted_iota(jnp.int32, query.shape, 1)
        zero = jnp.zeros_like(query)
        both = jnp.concatenate(
            [jnp.where(lane < HD, query, zero), jnp.where(lane < HD, zero, query)], axis=0
        )
        scores_ref[slot] = lax.dot_general(
            both, keys, LAST_DIMS, preferred_element_type=jnp.float32
        )

    def attend(step, slot):
        score = scores_ref[slot]
        top = jnp.max(score, axis=-1, keepdims=True)
        weight = jnp.exp2((score - top) * EXP_SCALE).astype(jnp.bfloat16)
        summed = jnp.dot(weight, values_ref[...], preferred_element_type=jnp.float32)
        first, second = summed[:rows], summed[rows:]
        head_out = first[:, :VD] / first[:, VD:] - lam * (second[:, :VD] / second[:, VD:])
        normed = head_out * lax.rsqrt(jnp.mean(head_out * head_out, axis=-1, keepdims=True) + eps)
        at = pl.ds(step * ATT_BLOCKS, ATT_BLOCKS)
        out_ref[at] = (
            (normed * gain * 0.8).astype(jnp.bfloat16).reshape(ATT_BLOCKS, tokens, VD)
        )

    scores(0, 0)
    for step in range(1, steps):
        scores(step, step % 2)
        attend(step - 1, (step - 1) % 2)
    attend(steps - 1, (steps - 1) % 2)
    fetch.wait()


def attention(lam, qkv, gain, out_weight, routes, experts):
    sources, _, tokens, width = qkv.shape
    length = sources * tokens
    in_vmem = pl.BlockSpec(memory_space=pltpu.VMEM)
    in_hbm = pl.BlockSpec(memory_space=pltpu.HBM)
    in_smem = pl.BlockSpec(memory_space=pltpu.SMEM)
    heads = (sources, tokens, VD)
    return pl.pallas_call(
        attention_kernel,
        in_specs=[in_smem, in_vmem, in_vmem, in_hbm, in_vmem],
        out_specs=[in_vmem] * 4,
        out_shape=[
            jax.ShapeDtypeStruct(heads, jnp.bfloat16),
            pltpu.VMEM(out_weight.shape, jnp.bfloat16),
            jax.ShapeDtypeStruct(routes.shape, jnp.int32),
            jax.ShapeDtypeStruct((CAP, experts), jnp.int32),
        ],
        scratch_shapes=[
            pltpu.VMEM((length, 2 * VD), jnp.bfloat16),
            pltpu.VMEM((2, 2 * ATT_BLOCKS * tokens, length), jnp.float32),
            pltpu.SemaphoreType.DMA((1,)),
        ],
        compiler_params=within(24),
        cost_estimate=pl.CostEstimate(
            flops=8 * length * length * VD,
            bytes_accessed=8 * length * VD,
            transcendentals=2 * length * length,
        ),
        name="attention",
    )(lam, on_chip(qkv), gain, off_chip(out_weight), routes)


ROW = (16, 128)
GROUP = 16
PAIR = 2 * GROUP
CAP = 4


def pack_kernel(query_ref, key_ref, value_ref, out_ref, rows, sems):
    copies = [
        pltpu.make_async_copy(ref, rows.at[at], sems.at[at])
        for at, ref in enumerate((query_ref, key_ref, value_ref))
    ]
    for copy in copies:
        copy.start()
    for at in range(3):
        copies[at].wait()
        for head in range(HEADS):
            out_ref[head, at] = rows[at, :, head * VD : (head + 1) * VD]


def pack_heads(query, key, value):
    tokens = query.shape[0]
    in_hbm = pl.BlockSpec(memory_space=pltpu.HBM)
    return pl.pallas_call(
        pack_kernel,
        in_specs=[in_hbm] * 3,
        out_specs=pl.BlockSpec(memory_space=pltpu.VMEM),
        out_shape=jax.ShapeDtypeStruct((HEADS, 3, tokens, VD), jnp.bfloat16),
        scratch_shapes=[
            pltpu.VMEM((3, tokens, HEADS * VD), jnp.bfloat16),
            pltpu.SemaphoreType.DMA((3,)),
        ],
        compiler_params=within(8),
        name="pack_heads",
    )(*(off_chip(a) for a in (query, key, value)))


def swap_matrix():
    size = GROUP * GROUP
    to = lax.broadcasted_iota(jnp.int32, (size, size), 0)
    at = lax.broadcasted_iota(jnp.int32, (size, size), 1)
    same = (to % GROUP) * GROUP + to // GROUP == at
    return jnp.where(same, 1.0, 0.0).astype(jnp.bfloat16)


def rows_to_tiles(rows, swap):
    halves = [
        jnp.concatenate(
            [rows[at : at + GROUP, 128 * j : 128 * (j + 1)] for j in range(16)], axis=0
        )
        for at in (0, GROUP)
    ]
    both = jnp.concatenate(halves, axis=1)
    swapped = jnp.dot(swap, both, preferred_element_type=jnp.float32).astype(jnp.bfloat16)
    return swapped[:, :128].reshape(GROUP, *ROW), swapped[:, 128:].reshape(GROUP, *ROW)


def tiles_to_rows(first, second, swap):
    size = GROUP * GROUP
    both = jnp.concatenate([first.reshape(size, 128), second.reshape(size, 128)], axis=1)
    swapped = jnp.dot(swap, both, preferred_element_type=jnp.float32).astype(jnp.bfloat16)
    return [
        jnp.concatenate(
            [swapped[GROUP * j : GROUP * (j + 1), at : at + 128] for j in range(16)], axis=1
        )
        for at in (0, 128)
    ]


def pair_slices(count):
    for at in range(0, count, PAIR):
        yield slice(at, at + GROUP), slice(at + GROUP, at + PAIR)


def middle_kernel(
    token_ref, heads_ref, weight_ref, residual_ref, gain_ref,
    mid_ref, sent_ref, heads_rows, middle, tiles,
):
    tokens = middle.shape[0]
    block = 512
    for head in range(HEADS):
        heads_rows[:, head * VD : (head + 1) * VD] = heads_ref[head]
    rows = heads_rows[...]
    squares = jnp.zeros((tokens, 128), jnp.float32)
    for at in range(0, D, block):
        columns = slice(at, at + block)
        projected = jnp.dot(rows, weight_ref[:, columns], preferred_element_type=jnp.float32)
        mid = (residual_ref[:, columns].astype(jnp.float32) + projected).astype(jnp.bfloat16)
        middle[:, columns] = mid
        wide = mid.astype(jnp.float32)
        wide = wide * wide
        for lane in range(0, block, 128):
            squares = squares + wide[:, lane : lane + 128]
    scale = lax.rsqrt(jnp.sum(squares, axis=-1, keepdims=True) / D + eps)
    swap = swap_matrix()
    for one, two in pair_slices(tokens):
        both = slice(one.start, two.stop)
        normed = middle[both, :].astype(jnp.float32) * scale[both] * gain_ref[...]
        tiles[one], tiles[two] = rows_to_tiles(normed.astype(jnp.bfloat16), swap)

    for index in range(sent_ref.shape[0]):
        sent_ref[index] = tiles[token_ref[index % CAP, index // CAP]]
    for one, two in pair_slices(tokens):
        mid_ref[one], mid_ref[two] = rows_to_tiles(middle[one.start : two.stop, :], swap)


def middle_stage(slot_token, heads, out_weight, residual, gain):
    tokens = residual.shape[0]
    slots = slot_token.size
    in_vmem = pl.BlockSpec(memory_space=pltpu.VMEM)
    return pl.pallas_call(
        middle_kernel,
        in_specs=[pl.BlockSpec(memory_space=pltpu.SMEM)] + [in_vmem] * 4,
        out_specs=[in_vmem] * 2,
        out_shape=[
            jax.ShapeDtypeStruct((tokens, *ROW), jnp.bfloat16),
            jax.ShapeDtypeStruct((slots, *ROW), jnp.bfloat16),
        ],
        scratch_shapes=[
            pltpu.VMEM((tokens, D), jnp.bfloat16),
            pltpu.VMEM((tokens, D), jnp.bfloat16),
            pltpu.VMEM((tokens, *ROW), jnp.bfloat16),
        ],
        compiler_params=within(16),
        cost_estimate=pl.CostEstimate(
            flops=2 * tokens * D * D, bytes_accessed=2 * D * D, transcendentals=0
        ),
        name="middle",
    )(slot_token, on_chip(heads), on_chip(out_weight), on_chip(residual), gain)


def expert_kernel(tile_ref, gate_ref, up_ref, down_ref, out_ref, rows, hidden, result):
    count = tile_ref.shape[0]
    block = 256
    swap = swap_matrix()
    for one, two in pair_slices(count):
        rows[one, :], rows[two, :] = tiles_to_rows(tile_ref[one], tile_ref[two], swap)
    inputs = rows[...]
    for at in range(0, hidden.shape[1], block):
        columns = slice(at, at + block)
        gate = jnp.dot(inputs, gate_ref[:, columns], preferred_element_type=jnp.float32)
        up = jnp.dot(inputs, up_ref[:, columns], preferred_element_type=jnp.float32)
        hidden[:, columns] = (gate / (1.0 + jnp.exp(-gate)) * up).astype(jnp.bfloat16)
    acts = hidden[...]
    for at in range(0, D, 1024):
        columns = slice(at, at + 1024)
        result[:, columns] = jnp.dot(
            acts, down_ref[:, columns], preferred_element_type=jnp.float32
        ).astype(jnp.bfloat16)
    for one, two in pair_slices(count):
        out_ref[one], out_ref[two] = rows_to_tiles(result[one.start : two.stop, :], swap)


def expert_stage(tiles, gate, up, down):
    count = tiles.shape[0]
    width = gate.shape[1]
    in_vmem = pl.BlockSpec(memory_space=pltpu.VMEM)
    return pl.pallas_call(
        expert_kernel,
        in_specs=[in_vmem] * 4,
        out_specs=in_vmem,
        out_shape=jax.ShapeDtypeStruct((count, *ROW), jnp.bfloat16),
        scratch_shapes=[
            pltpu.VMEM((count, D), jnp.bfloat16),
            pltpu.VMEM((count, width), jnp.bfloat16),
            pltpu.VMEM((count, D), jnp.bfloat16),
        ],
        compiler_params=within(24),
        cost_estimate=pl.CostEstimate(
            flops=6 * count * D * width, bytes_accessed=6 * D * width, transcendentals=0
        ),
        name="experts",
    )(on_chip(tiles), on_chip(gate), on_chip(up), on_chip(down))


def combine_kernel(slot_ref, share_ref, mid_ref, back_ref, out_hbm, tiles, out_ref, sems):
    tokens = mid_ref.shape[0]

    def token(index, carry):
        one = back_ref[slot_ref[0, index]].astype(jnp.float32) * share_ref[0, index]
        two = back_ref[slot_ref[1, index]].astype(jnp.float32) * share_ref[1, index]
        tiles[index] = (mid_ref[index].astype(jnp.float32) + (one + two)).astype(jnp.bfloat16)
        return carry

    swap = swap_matrix()
    copies = []
    for one, two in pair_slices(tokens):
        lax.fori_loop(one.start, two.stop, token, 0, unroll=PAIR)
        out_ref[one, :], out_ref[two, :] = tiles_to_rows(tiles[one], tiles[two], swap)
        at = pl.ds(one.start, PAIR)
        copy = pltpu.make_async_copy(out_ref.at[at], out_hbm.at[at], sems.at[len(copies)])
        copy.start()
        copies.append(copy)
    for copy in copies:
        copy.wait()


def combine_stage(slot, shares, mid, back):
    tokens = mid.shape[0]
    in_smem = pl.BlockSpec(memory_space=pltpu.SMEM)
    in_vmem = pl.BlockSpec(memory_space=pltpu.VMEM)
    return pl.pallas_call(
        combine_kernel,
        in_specs=[in_smem, in_smem, in_vmem, in_vmem],
        out_specs=pl.BlockSpec(memory_space=pltpu.HBM),
        out_shape=pltpu.HBM((tokens, D), jnp.bfloat16),
        scratch_shapes=[
            pltpu.VMEM((tokens, *ROW), jnp.bfloat16),
            pltpu.VMEM((tokens, D), jnp.bfloat16),
            pltpu.SemaphoreType.DMA((tokens // PAIR,)),
        ],
        compiler_params=within(8),
        name="combine",
    )(slot, shares, on_chip(mid), on_chip(back))


def on_device(
    residual,
    query_maps,
    key_maps,
    value_rows,
    lambdas,
    head_gain,
    out_weight,
    ffn_gain,
    routes,
    route_weights,
    expert_gate,
    expert_up,
    expert_down,
):
    count_sp = lax.axis_size(SP)
    count_dp = lax.axis_size("dp")
    packed = pack_heads(query_maps[0], key_maps[0], value_rows[0])
    qkv = lax.all_to_all(packed, SP, split_axis=0, concat_axis=0, tiled=True)
    experts_all = count_sp * count_dp
    attended, weight_here, slot, slot_token = attention(
        lambdas, qkv, head_gain.reshape(HEADS, VD), out_weight, routes[0].T, experts_all
    )
    returned = lax.all_to_all(attended, SP, split_axis=0, concat_axis=0, tiled=True)
    mid, sent = middle_stage(slot_token, returned, weight_here, residual[0], ffn_gain[None])
    arrived = lax.all_to_all(sent, SP_DP, split_axis=0, concat_axis=0, tiled=True)
    done = expert_stage(arrived, expert_gate[0], expert_up[0], expert_down[0])
    back = lax.all_to_all(done, SP_DP, split_axis=0, concat_axis=0, tiled=True)
    return combine_stage(slot, route_weights[0].T, mid, back)[None]


def solution(mesh):
    finer = Mesh(mesh.devices.reshape(4, 4, mesh.shape["dp"]), ("sp_0", "sp_1", "dp"))
    placed = (
        P("dp", SP, None),
        P("dp", SP, None),
        P("dp", SP, None),
        P("dp", SP, None),
        P(),
        P(),
        P(),
        P(),
        P("dp", SP, None),
        P("dp", SP, None),
        P(SP_DP, None, None),
        P(SP_DP, None, None),
        P(SP_DP, None, None),
    )
    return jax.shard_map(
        on_device, mesh=finer, in_specs=placed, out_specs=P("dp", SP, None), check_vma=False
    )
```

```python
import math

import jax
import jax.numpy as jnp
from jax import lax
from jax.experimental import pallas as pl
from jax.experimental.pallas import tpu as pltpu
from jax.sharding import Mesh
from jax.sharding import PartitionSpec as P

D = 2048
HEADS = 16
HD = 64
VD = 128
SP = ("sp_0", "sp_1")
SP_DP = ("sp_0", "sp_1", "dp")


eps = 1e-06


def on_chip(value):
    return pltpu.with_memory_space_constraint(value, pltpu.VMEM)


def off_chip(value):
    return pltpu.with_memory_space_constraint(value, pltpu.HBM)


def within(mebibytes):
    return pltpu.CompilerParams(vmem_limit_bytes=mebibytes * 2**20)


EXP_SCALE = HD ** (-0.5) * math.log2(math.e)
LAST_DIMS = (((1,), (1,)), ((), ()))
ATT_BLOCKS = 2


def route_rows(routes_ref, slot_ref, token_ref):
    experts = token_ref.shape[1]
    topk, tokens = routes_ref.shape
    expert_at = lax.broadcasted_iota(jnp.int32, (experts, tokens), 0)
    square = (tokens, tokens)
    earlier = lax.broadcasted_iota(jnp.int32, square, 0) < lax.broadcasted_iota(
        jnp.int32, square, 1
    )
    earlier = jnp.where(earlier, 1.0, 0.0).astype(jnp.bfloat16)
    taken = jnp.zeros((experts, 1), jnp.float32)
    ranked = [jnp.zeros((experts, tokens), jnp.float32) for _ in range(CAP)]
    for k in range(topk):
        here = jnp.where(expert_at == routes_ref[k : k + 1, :], 1.0, 0.0)
        before = taken + jnp.dot(
            here.astype(jnp.bfloat16), earlier, preferred_element_type=jnp.float32
        )
        slot = here * (CAP * expert_at.astype(jnp.float32) + before)
        slot_ref[k : k + 1, :] = jnp.sum(slot, axis=0, keepdims=True).astype(jnp.int32)
        taken = taken + jnp.sum(here, axis=1, keepdims=True)
        for rank in range(CAP):
            ranked[rank] = ranked[rank] + jnp.where(before == rank, here, 0.0)
    token_at = lax.broadcasted_iota(jnp.int32, (16, tokens), 1).astype(jnp.float32)
    for rank in range(CAP):
        of_slot = lax.dot_general(
            token_at.astype(jnp.bfloat16),
            ranked[rank].astype(jnp.bfloat16),
            LAST_DIMS,
            preferred_element_type=jnp.float32,
        )
        token_ref[rank : rank + 1, :] = of_slot[:1].astype(jnp.int32)


def attention_kernel(
    lam_ref, qkv_ref, gain_ref, weight_hbm,
    out_ref, weight_ref, values_ref, scores_ref, sems,
):
    head = lax.axis_index(SP)
    lam = lam_ref[head]
    gain = gain_ref[pl.ds(head, 1), :]
    sources, _, tokens, width = qkv_ref.shape
    length = sources * tokens
    rows = ATT_BLOCKS * tokens
    steps = sources // ATT_BLOCKS
    fetch = pltpu.make_async_copy(weight_hbm, weight_ref, sems.at[0])
    fetch.start()
    values_ref[:, :VD] = qkv_ref[:, 2].reshape(length, width)
    values_ref[:, VD:] = jnp.ones((length, VD), jnp.bfloat16)

    def scores(step, slot):
        keys = qkv_ref[:, 1].reshape(length, width)
        query = qkv_ref[pl.ds(step * ATT_BLOCKS, ATT_BLOCKS), 0].reshape(rows, width)
        lane = lax.broadcasted_iota(jnp.int32, query.shape, 1)
        zero = jnp.zeros_like(query)
        both = jnp.concatenate(
            [jnp.where(lane < HD, query, zero), jnp.where(lane < HD, zero, query)], axis=0
        )
        scores_ref[slot] = lax.dot_general(
            both, keys, LAST_DIMS, preferred_element_type=jnp.float32
        )

    def attend(step, slot):
        score = scores_ref[slot]
        top = jnp.max(score, axis=-1, keepdims=True)
        weight = jnp.exp2((score - top) * EXP_SCALE).astype(jnp.bfloat16)
        summed = jnp.dot(weight, values_ref[...], preferred_element_type=jnp.float32)
        first, second = summed[:rows], summed[rows:]
        head_out = first[:, :VD] / first[:, VD:] - lam * (second[:, :VD] / second[:, VD:])
        normed = head_out * lax.rsqrt(jnp.mean(head_out * head_out, axis=-1, keepdims=True) + eps)
        at = pl.ds(step * ATT_BLOCKS, ATT_BLOCKS)
        out_ref[at] = (
            (normed * gain * 0.8).astype(jnp.bfloat16).reshape(ATT_BLOCKS, tokens, VD)
        )

    scores(0, 0)
    for step in range(1, steps):
        scores(step, step % 2)
        attend(step - 1, (step - 1) % 2)
    attend(steps - 1, (steps - 1) % 2)
    fetch.wait()


def attention(lam, qkv, gain, out_weight):
    sources, _, tokens, width = qkv.shape
    length = sources * tokens
    in_vmem = pl.BlockSpec(memory_space=pltpu.VMEM)
    in_hbm = pl.BlockSpec(memory_space=pltpu.HBM)
    in_smem = pl.BlockSpec(memory_space=pltpu.SMEM)
    heads = (sources, tokens, VD)
    return pl.pallas_call(
        attention_kernel,
        in_specs=[in_smem, in_vmem, in_vmem, in_hbm],
        out_specs=[in_vmem] * 2,
        out_shape=[
            jax.ShapeDtypeStruct(heads, jnp.bfloat16),
            pltpu.VMEM(out_weight.shape, jnp.bfloat16),
        ],
        scratch_shapes=[
            pltpu.VMEM((length, 2 * VD), jnp.bfloat16),
            pltpu.VMEM((2, 2 * ATT_BLOCKS * tokens, length), jnp.float32),
            pltpu.SemaphoreType.DMA((1,)),
        ],
        compiler_params=within(24),
        cost_estimate=pl.CostEstimate(
            flops=8 * length * length * VD,
            bytes_accessed=8 * length * VD,
            transcendentals=2 * length * length,
        ),
        name="attention",
    )(lam, on_chip(qkv), gain, off_chip(out_weight))


ROW = (16, 128)
GROUP = 16
PAIR = 2 * GROUP
CAP = 4


def pack_kernel(
    routes_hbm, query_ref, key_ref, value_ref,
    out_ref, slot_ref, token_ref, routes_ref, rows, sems,
):
    route_copy = pltpu.make_async_copy(routes_hbm, routes_ref, sems.at[3])
    copies = [
        pltpu.make_async_copy(ref, rows.at[at], sems.at[at])
        for at, ref in enumerate((query_ref, key_ref, value_ref))
    ]
    route_copy.start()
    for copy in copies:
        copy.start()
    route_copy.wait()
    route_rows(routes_ref, slot_ref, token_ref)
    for at in range(3):
        copies[at].wait()
        for head in range(HEADS):
            out_ref[head, at] = rows[at, :, head * VD : (head + 1) * VD]


def pack_heads(routes, query, key, value, experts):
    tokens = query.shape[0]
    in_hbm = pl.BlockSpec(memory_space=pltpu.HBM)
    in_vmem = pl.BlockSpec(memory_space=pltpu.VMEM)
    return pl.pallas_call(
        pack_kernel,
        in_specs=[in_hbm] * 4,
        out_specs=[in_vmem] * 3,
        out_shape=[
            jax.ShapeDtypeStruct((HEADS, 3, tokens, VD), jnp.bfloat16),
            jax.ShapeDtypeStruct(routes.shape, jnp.int32),
            jax.ShapeDtypeStruct((CAP, experts), jnp.int32),
        ],
        scratch_shapes=[
            pltpu.VMEM(routes.shape, jnp.int32),
            pltpu.VMEM((3, tokens, HEADS * VD), jnp.bfloat16),
            pltpu.SemaphoreType.DMA((4,)),
        ],
        compiler_params=within(8),
        name="pack_heads",
    )(*(off_chip(a) for a in (routes, query, key, value)))


def swap_matrix():
    size = GROUP * GROUP
    to = lax.broadcasted_iota(jnp.int32, (size, size), 0)
    at = lax.broadcasted_iota(jnp.int32, (size, size), 1)
    same = (to % GROUP) * GROUP + to // GROUP == at
    return jnp.where(same, 1.0, 0.0).astype(jnp.bfloat16)


def rows_to_tiles(rows, swap):
    halves = [
        jnp.concatenate(
            [rows[at : at + GROUP, 128 * j : 128 * (j + 1)] for j in range(16)], axis=0
        )
        for at in (0, GROUP)
    ]
    both = jnp.concatenate(halves, axis=1)
    swapped = jnp.dot(swap, both, preferred_element_type=jnp.float32).astype(jnp.bfloat16)
    return swapped[:, :128].reshape(GROUP, *ROW), swapped[:, 128:].reshape(GROUP, *ROW)


def tiles_to_rows(first, second, swap):
    size = GROUP * GROUP
    both = jnp.concatenate([first.reshape(size, 128), second.reshape(size, 128)], axis=1)
    swapped = jnp.dot(swap, both, preferred_element_type=jnp.float32).astype(jnp.bfloat16)
    return [
        jnp.concatenate(
            [swapped[GROUP * j : GROUP * (j + 1), at : at + 128] for j in range(16)], axis=1
        )
        for at in (0, 128)
    ]


def pair_slices(count):
    for at in range(0, count, PAIR):
        yield slice(at, at + GROUP), slice(at + GROUP, at + PAIR)


def middle_kernel(
    token_ref, heads_ref, weight_ref, residual_ref, gain_ref,
    mid_ref, sent_ref, heads_rows, middle, tiles,
):
    tokens = middle.shape[0]
    block = 512
    for head in range(HEADS):
        heads_rows[:, head * VD : (head + 1) * VD] = heads_ref[head]
    rows = heads_rows[...]
    squares = jnp.zeros((tokens, 128), jnp.float32)
    for at in range(0, D, block):
        columns = slice(at, at + block)
        projected = jnp.dot(rows, weight_ref[:, columns], preferred_element_type=jnp.float32)
        mid = (residual_ref[:, columns].astype(jnp.float32) + projected).astype(jnp.bfloat16)
        middle[:, columns] = mid
        wide = mid.astype(jnp.float32)
        wide = wide * wide
        for lane in range(0, block, 128):
            squares = squares + wide[:, lane : lane + 128]
    scale = lax.rsqrt(jnp.sum(squares, axis=-1, keepdims=True) / D + eps)
    swap = swap_matrix()
    for one, two in pair_slices(tokens):
        both = slice(one.start, two.stop)
        normed = middle[both, :].astype(jnp.float32) * scale[both] * gain_ref[...]
        tiles[one], tiles[two] = rows_to_tiles(normed.astype(jnp.bfloat16), swap)

    for index in range(sent_ref.shape[0]):
        sent_ref[index] = tiles[token_ref[index % CAP, index // CAP]]
    for one, two in pair_slices(tokens):
        mid_ref[one], mid_ref[two] = rows_to_tiles(middle[one.start : two.stop, :], swap)


def middle_stage(slot_token, heads, out_weight, residual, gain):
    tokens = residual.shape[0]
    slots = slot_token.size
    in_vmem = pl.BlockSpec(memory_space=pltpu.VMEM)
    return pl.pallas_call(
        middle_kernel,
        in_specs=[pl.BlockSpec(memory_space=pltpu.SMEM)] + [in_vmem] * 4,
        out_specs=[in_vmem] * 2,
        out_shape=[
            jax.ShapeDtypeStruct((tokens, *ROW), jnp.bfloat16),
            jax.ShapeDtypeStruct((slots, *ROW), jnp.bfloat16),
        ],
        scratch_shapes=[
            pltpu.VMEM((tokens, D), jnp.bfloat16),
            pltpu.VMEM((tokens, D), jnp.bfloat16),
            pltpu.VMEM((tokens, *ROW), jnp.bfloat16),
        ],
        compiler_params=within(16),
        cost_estimate=pl.CostEstimate(
            flops=2 * tokens * D * D, bytes_accessed=2 * D * D, transcendentals=0
        ),
        name="middle",
    )(slot_token, on_chip(heads), on_chip(out_weight), on_chip(residual), gain)


def expert_kernel(tile_ref, gate_ref, up_ref, down_ref, out_ref, rows, hidden, result):
    count = tile_ref.shape[0]
    block = 256
    swap = swap_matrix()
    for one, two in pair_slices(count):
        rows[one, :], rows[two, :] = tiles_to_rows(tile_ref[one], tile_ref[two], swap)
    inputs = rows[...]
    for at in range(0, hidden.shape[1], block):
        columns = slice(at, at + block)
        gate = jnp.dot(inputs, gate_ref[:, columns], preferred_element_type=jnp.float32)
        up = jnp.dot(inputs, up_ref[:, columns], preferred_element_type=jnp.float32)
        hidden[:, columns] = (gate / (1.0 + jnp.exp(-gate)) * up).astype(jnp.bfloat16)
    acts = hidden[...]
    for at in range(0, D, 1024):
        columns = slice(at, at + 1024)
        result[:, columns] = jnp.dot(
            acts, down_ref[:, columns], preferred_element_type=jnp.float32
        ).astype(jnp.bfloat16)
    for one, two in pair_slices(count):
        out_ref[one], out_ref[two] = rows_to_tiles(result[one.start : two.stop, :], swap)


def expert_stage(tiles, gate, up, down):
    count = tiles.shape[0]
    width = gate.shape[1]
    in_vmem = pl.BlockSpec(memory_space=pltpu.VMEM)
    return pl.pallas_call(
        expert_kernel,
        in_specs=[in_vmem] * 4,
        out_specs=in_vmem,
        out_shape=jax.ShapeDtypeStruct((count, *ROW), jnp.bfloat16),
        scratch_shapes=[
            pltpu.VMEM((count, D), jnp.bfloat16),
            pltpu.VMEM((count, width), jnp.bfloat16),
            pltpu.VMEM((count, D), jnp.bfloat16),
        ],
        compiler_params=within(24),
        cost_estimate=pl.CostEstimate(
            flops=6 * count * D * width, bytes_accessed=6 * D * width, transcendentals=0
        ),
        name="experts",
    )(on_chip(tiles), on_chip(gate), on_chip(up), on_chip(down))


def combine_kernel(slot_ref, share_ref, mid_ref, back_ref, out_hbm, tiles, out_ref, sems):
    tokens = mid_ref.shape[0]

    def token(index, carry):
        one = back_ref[slot_ref[0, index]].astype(jnp.float32) * share_ref[0, index]
        two = back_ref[slot_ref[1, index]].astype(jnp.float32) * share_ref[1, index]
        tiles[index] = (mid_ref[index].astype(jnp.float32) + (one + two)).astype(jnp.bfloat16)
        return carry

    swap = swap_matrix()
    copies = []
    for one, two in pair_slices(tokens):
        lax.fori_loop(one.start, two.stop, token, 0, unroll=PAIR)
        out_ref[one, :], out_ref[two, :] = tiles_to_rows(tiles[one], tiles[two], swap)
        at = pl.ds(one.start, PAIR)
        copy = pltpu.make_async_copy(out_ref.at[at], out_hbm.at[at], sems.at[len(copies)])
        copy.start()
        copies.append(copy)
    for copy in copies:
        copy.wait()


def combine_stage(slot, shares, mid, back):
    tokens = mid.shape[0]
    in_smem = pl.BlockSpec(memory_space=pltpu.SMEM)
    in_vmem = pl.BlockSpec(memory_space=pltpu.VMEM)
    return pl.pallas_call(
        combine_kernel,
        in_specs=[in_smem, in_smem, in_vmem, in_vmem],
        out_specs=pl.BlockSpec(memory_space=pltpu.HBM),
        out_shape=pltpu.HBM((tokens, D), jnp.bfloat16),
        scratch_shapes=[
            pltpu.VMEM((tokens, *ROW), jnp.bfloat16),
            pltpu.VMEM((tokens, D), jnp.bfloat16),
            pltpu.SemaphoreType.DMA((tokens // PAIR,)),
        ],
        compiler_params=within(8),
        name="combine",
    )(slot, shares, on_chip(mid), on_chip(back))


def on_device(
    residual,
    query_maps,
    key_maps,
    value_rows,
    lambdas,
    head_gain,
    out_weight,
    ffn_gain,
    routes,
    route_weights,
    expert_gate,
    expert_up,
    expert_down,
):
    count_sp = lax.axis_size(SP)
    count_dp = lax.axis_size("dp")
    packed, slot, slot_token = pack_heads(
        routes[0].T, query_maps[0], key_maps[0], value_rows[0], count_sp * count_dp
    )
    qkv = lax.all_to_all(packed, SP, split_axis=0, concat_axis=0, tiled=True)
    attended, weight_here = attention(lambdas, qkv, head_gain.reshape(HEADS, VD), out_weight)
    returned = lax.all_to_all(attended, SP, split_axis=0, concat_axis=0, tiled=True)
    mid, sent = middle_stage(slot_token, returned, weight_here, residual[0], ffn_gain[None])
    arrived = lax.all_to_all(sent, SP_DP, split_axis=0, concat_axis=0, tiled=True)
    done = expert_stage(arrived, expert_gate[0], expert_up[0], expert_down[0])
    back = lax.all_to_all(done, SP_DP, split_axis=0, concat_axis=0, tiled=True)
    return combine_stage(slot, route_weights[0].T, mid, back)[None]


def solution(mesh):
    finer = Mesh(mesh.devices.reshape(4, 4, mesh.shape["dp"]), ("sp_0", "sp_1", "dp"))
    placed = (
        P("dp", SP, None),
        P("dp", SP, None),
        P("dp", SP, None),
        P("dp", SP, None),
        P(),
        P(),
        P(),
        P(),
        P("dp", SP, None),
        P("dp", SP, None),
        P(SP_DP, None, None),
        P(SP_DP, None, None),
        P(SP_DP, None, None),
    )
    return jax.shard_map(
        on_device, mesh=finer, in_specs=placed, out_specs=P("dp", SP, None), check_vma=False
    )
```
